512 devices in a mesh: sp: 64 (over z, y), tp: 8 (over x, core).
Axes of the slice: x: 4, y: 4, z: 16, core: 2. Of those that a mesh axis runs over, the one named last changes fastest.
Arguments:
- queries: bfloat16 [8192, 768], P('sp', 'tp'), may hold values from -6 to 6
- latents: bfloat16 [8192, 512], P('sp'), may hold values from -6 to 6
- rot_key: bfloat16 [8192, 32], P('sp'), may hold values from -6 to 6
- kv_weight: bfloat16 [512, 1024], P(None, 'tp'), may hold values from -0.25 to 0.25
- log_sums: float32 [8192, 8], P('sp', 'tp'), may hold values from 4 to 14, as said below
- outputs: bfloat16 [8192, 512], P('sp', 'tp'), may hold values from -4 to 4
- out_grad: bfloat16 [8192, 512], P('sp', 'tp'), may hold values from -384 to 384
Outputs:
- query_grad: bfloat16 [8192, 768], P('sp', 'tp')
- key_grad: bfloat16 [8192, 512], P('sp', 'tp')
- value_grad: bfloat16 [8192, 512], P('sp', 'tp')
- rot_grad: float32 [8192, 32], P('sp')
- weight_grad: float32 [512, 1024], P('sp', 'tp')
The draws below stay inside these ranges and needn't reach their ends.
Inputs may be any that keep to these rules, and one draw needn't show every extreme that they name: `log_sums`: each value lies within one half of log(8192) + 0.5.
All inputs are finite; a program needn't handle non-finite values.
Results may differ from the reference program's by a relative error of at most 0.004.
The reference program's roundings to bfloat16 on the way (of `joined`, `key_full`, `probs_b` and `dscore`) count: a program that leaves them out, or rounds other values in their place, can miss the bound.
Values may be sent and summed in bfloat16 or wider, within the bound.
A program may use at most 64 MiB of HBM per device.

```python
import math
import jax
import jax.numpy as jnp
from jax import lax

HEADS = 8
RANK = 512
NOPE_DIM = 64
ROPE_DIM = 32
VALUE_DIM = 64
SEQ = 8192


def draw_log_sums(key, part):
    center = math.log(SEQ) + 0.5
    return center + jax.random.uniform(key, (SEQ, HEADS), jnp.float32, -0.5, 0.5)


def with_spikes(result, own_key, source, target, parts, factor):
    def block_of(dim):
        return (jnp.arange(result.shape[dim]) // (result.shape[dim] // parts)).reshape((-1,) + (1,) * (result.ndim - 1 - dim))

    near = jax.random.permutation(own_key, parts)[block_of(target)]
    other_side = (block_of(target) + parts // 2) % parts
    return jnp.where((block_of(source) == near) | (block_of(source) == other_side), factor * result, result)


def block_scale(rng, dims, split, low, top_value):
    def one(dim, blocks):
        draws = jax.random.uniform(jax.random.fold_in(jax.random.fold_in(rng, 6), dim), (blocks,), jnp.float32, low / len(split), top_value / len(split))
        return jnp.repeat(jnp.exp(draws), dims[dim] // blocks).reshape((-1,) + (1,) * (len(dims) - dim - 1))

    loudness = one(*split[0])
    for cut in split[1:]:
        loudness = loudness * one(*cut)
    return loudness


def normal_values(key, shape, deviation, reach, shards=(), kind=jnp.bfloat16):
    array = jax.random.normal(key, shape, jnp.float32) * deviation
    if len(shards) > 0:
        array = block_scale(key, shape, shards, -0.22, 0.18) * array
    return jnp.clip(array, min=-reach, max=reach).astype(kind)


def noise_with(own_key, extent, spread, limit, pieces, heavy, held_as=jnp.bfloat16):
    entries = spread * jax.random.normal(own_key, extent, jnp.float32)
    if pieces:
        entries = entries * block_scale(own_key, extent, pieces, -0.22, 0.18)
    return jnp.clip(with_spikes(entries, jax.random.fold_in(own_key, 3), *heavy), -limit, limit).astype(held_as)


def setup_inputs(seed: int = 0) -> dict:
    splits = jax.random.split(jax.random.key(seed), 8)
    queries = normal_values(splits[0], (SEQ, HEADS * (NOPE_DIM + ROPE_DIM)), 1.0, 6.0, ((0, 64), (1, 8)))
    latents = normal_values(splits[1], (SEQ, RANK), 1.0, 6.0, ((0, 64),))
    rot_key = normal_values(splits[2], (SEQ, ROPE_DIM), 1.0, 6.0, ((0, 64),))
    kv_weight = normal_values(splits[3], (RANK, HEADS * (NOPE_DIM + VALUE_DIM)), RANK ** -0.5, 0.25, ((1, 8),))
    log_sums = draw_log_sums(jax.random.fold_in(splits[7], 71), 0)
    outputs = normal_values(splits[5], (SEQ, HEADS * VALUE_DIM), 0.3, 4.0, ((0, 64), (1, 8)))
    out_grad = noise_with(splits[6], (SEQ, HEADS * VALUE_DIM), (SEQ ** 0.5 / 4), 384.0, ((0, 64), (1, 8)), (0, 1, 64, 4.0))
    return dict(queries=queries, latents=latents, rot_key=rot_key, kv_weight=kv_weight, log_sums=log_sums, outputs=outputs, out_grad=out_grad)


def round_keep(values):
    rounded = values.astype(jnp.bfloat16)
    rounded = lax.optimization_barrier(rounded)
    return rounded.astype(jnp.float32)


def reference(queries, latents, rot_key, kv_weight, log_sums, outputs, out_grad):
    head_dim = NOPE_DIM + ROPE_DIM
    score_scale = head_dim ** -0.5
    joined = jnp.dot(latents, kv_weight, preferred_element_type=jnp.float32).astype(jnp.bfloat16)
    joined = joined.reshape(SEQ, HEADS, NOPE_DIM + VALUE_DIM).astype(jnp.float32)
    rotary = jnp.broadcast_to(rot_key.astype(jnp.float32)[:, None, :], (SEQ, HEADS, ROPE_DIM))
    key_full = jnp.concatenate([joined[:, :, :NOPE_DIM], rotary], axis=-1)
    values = joined[:, :, NOPE_DIM:]
    query_full = queries.astype(jnp.float32).reshape(SEQ, HEADS, head_dim)
    grad_full = out_grad.astype(jnp.float32).reshape(SEQ, HEADS, VALUE_DIM)
    row_delta = jnp.sum(outputs.astype(jnp.float32).reshape(SEQ, HEADS, VALUE_DIM) * grad_full, axis=-1)
    block_rows = math.gcd(SEQ, 512)
    block_count = SEQ // block_rows

    def block_step(totals, block_index):
        key_total, value_total = totals
        begin_row = (block_index * block_rows).astype(jnp.int32)
        query_block = lax.dynamic_slice_in_dim(query_full, begin_row, block_rows, 0)
        grad_block = lax.dynamic_slice_in_dim(grad_full, begin_row, block_rows, 0)
        log_block = lax.dynamic_slice_in_dim(log_sums, begin_row, block_rows, 0)
        delta_block = lax.dynamic_slice_in_dim(row_delta, begin_row, block_rows, 0)
        scores = jnp.einsum('qhd,khd->hqk', query_block, key_full) * score_scale
        probs = jnp.exp(scores - log_block.T[:, :, None])
        dprob = jnp.einsum('qhd,khd->hqk', grad_block, values)
        dscore = round_keep(probs * (dprob - delta_block.T[:, :, None]))
        probs_b = round_keep(probs)
        query_part = (jnp.einsum('hqk,khd->qhd', dscore, key_full) * score_scale).astype(jnp.bfloat16)
        key_total = key_total + jnp.einsum('hqk,qhd->khd', dscore, query_block) * score_scale
        value_total = value_total + jnp.einsum('hqk,qhd->khd', probs_b, grad_block)
        return (key_total, value_total), query_part

    start_totals = (jnp.zeros((SEQ, HEADS, head_dim), jnp.float32), jnp.zeros((SEQ, HEADS, VALUE_DIM), jnp.float32))
    (key_total, value_total), query_blocks = lax.scan(block_step, start_totals, jnp.arange(block_count, dtype=jnp.int32))
    query_grad = query_blocks.reshape(SEQ, HEADS * head_dim)
    rot_grad = jnp.sum(key_total[:, :, NOPE_DIM:], axis=1)
    key_grad = key_total[:, :, :NOPE_DIM].astype(jnp.bfloat16)
    value_grad = value_total.astype(jnp.bfloat16)
    stacked = jnp.concatenate([key_grad, value_grad], axis=-1).reshape(SEQ, HEADS * (NOPE_DIM + VALUE_DIM))
    weight_grad = jnp.dot(latents.T, stacked, preferred_element_type=jnp.float32)
    return (query_grad, key_grad.reshape(SEQ, HEADS * NOPE_DIM), value_grad.reshape(SEQ, HEADS * VALUE_DIM), rot_grad, weight_grad)
```

```python
import jax
import jax.numpy as jnp
from jax import lax
from jax.experimental import pallas as pl
from jax.experimental.pallas import tpu as pltpu
from jax.sharding import PartitionSpec as P

MESH = pl.DeviceIdType.MESH
F32 = jnp.float32
BF16 = jnp.bfloat16

NOPE = 64
ROPE = 32
VAL = 64
RANK = 512
ROWS = 128
NY = 4
NZ = 16
NTP = 8
PACK = 176
SCALE = (NOPE + ROPE) ** -0.5
LOG2E = 1.4426950408889634

Q_FAR = 0
Q_Y = 3
KV = 15
LAT = 18
DQ_Y = 21
DQ_Z = 33
DKV = 36
DROT = 39
W_Y = 42
W_Z = 45
ROT = 60
COPIES = 67


def three(x):
    hi = x.astype(BF16)
    rest = x - hi.astype(F32)
    mid = rest.astype(BF16)
    low = (rest - mid.astype(F32)).astype(BF16)
    return [hi.astype(F32), mid.astype(F32), low.astype(F32)]


def dot(a, b):
    return jnp.dot(a, b, preferred_element_type=F32)


def dot_nt(a, b):
    return lax.dot_general(a, b, (((1,), (1,)), ((), ())), preferred_element_type=F32)


def kernel(
    q_ref, lat_ref, rot_ref, w_ref, lse_ref, o_ref, do_ref,
    dq_ref, dk_ref, dv_ref, drot_ref, dw_ref,
    qbuf, kvbuf, kt, latt, mbuf, acc, dqp, dqr, dqs, dqz, dkvs, dkvr, rots, rotr, rotx, wsend, wrecv, wzs, wzr,
    ssem, rsem,
):
    sp = lax.axis_index("sp")
    tp = lax.axis_index("tp")
    z = sp // NY
    y = sp % NY
    odd = z % 2
    sign = 1 - 2 * odd

    def dev(dz, dy):
        return (((z + dz + NZ) % NZ) * NY + (y + dy + NY) % NY, tp)

    y_off = (0, 1, -1, 2)
    k_off = (0, 1, -1, 2 * sign)

    def copy(number, src, dst, device):
        return pltpu.make_async_remote_copy(
            src_ref=src, dst_ref=dst, send_sem=ssem.at[number], recv_sem=rsem.at[number],
            device_id=device, device_id_type=MESH,
        )

    barrier = pltpu.get_barrier_semaphore()
    greet = [dev(d, 0) for d in (1, -1, 2, -2, 4, -4)] + [dev(0, d) for d in (1, -1, 2)]
    greet += [(sp, (tp + k) % NTP) for k in range(1, NTP)]
    for device in greet:
        pl.semaphore_signal(barrier, inc=1, device_id=device, device_id_type=MESH)

    q_t = jnp.transpose(q_ref[...].astype(F32))
    do = do_ref[...].astype(F32)
    do_t = jnp.transpose(do)
    o_t = jnp.transpose(o_ref[...].astype(F32))
    delta = jnp.sum(o_t * do_t, axis=0, keepdims=True)
    lse = jnp.transpose(jnp.broadcast_to(lse_ref[...], (ROWS, ROWS)))[0:1] * (1.0 / SCALE)
    row = lax.broadcasted_iota(jnp.int32, (16, ROWS), 0)
    aux = jnp.zeros((16, ROWS), F32)
    for i, piece in enumerate(three(lse) + three(delta)):
        aux = jnp.where(row == i, jnp.broadcast_to(piece, (16, ROWS)), aux)
    qbuf[0, 0:64, :] = q_t[0:64].astype(BF16)
    qbuf[0, 64:128, :] = do_t.astype(BF16)
    qbuf[0, 128:160, :] = q_t[64:96].astype(BF16)
    qbuf[0, 160:176, :] = aux.astype(BF16)

    pl.semaphore_wait(barrier, len(greet))

    q_far = [
        copy(Q_FAR + 0, qbuf.at[0], qbuf.at[8], dev(-4, 0)),
        copy(Q_FAR + 1, qbuf.at[0], qbuf.at[4], dev(4, 0)),
        copy(Q_FAR + 2, qbuf.at[4 + 4 * odd], qbuf.at[12], dev(4 * sign, 0)),
    ]
    q_far[0].start()
    q_far[1].start()
    q_y = [
        [copy(Q_Y + 3 * t + u - 1, qbuf.at[4 * t], qbuf.at[4 * t + u], dev(0, y_off[u])) for u in (1, 2, 3)]
        for t in range(4)
    ]
    for c in q_y[0]:
        c.start()

    joined = dot(lat_ref[...], w_ref[...]).astype(BF16)
    kvbuf[0:ROWS, 0:128] = joined
    lane = lax.broadcasted_iota(jnp.int32, (ROWS, 128), 1)
    kvbuf[0:ROWS, 128:256] = jnp.where((lane >= ROPE) & (lane < ROPE + 6), -1.0, 0.0).astype(BF16)
    kvbuf[0:ROWS, 128 : 128 + ROPE] = rot_ref[...]

    def rows_of(s):
        return pl.ds(ROWS * s, ROWS)

    kv = [copy(KV + s - 1, kvbuf.at[rows_of(0)], kvbuf.at[rows_of(s)], dev(k_off[s], 0)) for s in (1, 2, 3)]
    for c in kv:
        c.start()
    latt[0] = jnp.transpose(lat_ref[...].astype(F32)).astype(BF16)
    lat = [copy(LAT + s - 1, latt.at[0], latt.at[s], dev(k_off[s], 0)) for s in (1, 2, 3)]
    for c in lat:
        c.start()

    mbuf[...] = jnp.zeros_like(mbuf)
    acc[...] = jnp.zeros_like(acc)

    for c in kv:
        c.wait_recv()
    kt[0:64, :] = jnp.transpose(kvbuf[:, 0:128].astype(F32))[0:64].astype(BF16)
    kt[64:96, :] = jnp.transpose(kvbuf[:, 128:256].astype(F32))[0:32].astype(BF16)

    def process(slot):
        mbuf[0:64, 0:128] = qbuf[slot, 0:64, :]
        mbuf[64:128, 128:256] = qbuf[slot, 64:128, :]
        mbuf[128:160, 0:128] = qbuf[slot, 128:160, :]
        extra = qbuf[slot, 160:176, :].astype(F32)
        mbuf[160:176, 0:128] = jnp.where(row < 3, extra, 0.0).astype(BF16)
        mbuf[160:176, 128:256] = jnp.where(row >= 3, extra, 0.0).astype(BF16)
        m = mbuf[...]
        total = jnp.zeros((96, ROWS), F32)
        for c in range(2):
            rows = pl.ds(256 * c, 256)
            both = dot(kvbuf[rows, :], m)
            probs = jnp.exp2(both[:, 0:128] * (SCALE * LOG2E))
            ds = (probs * both[:, 128:256]).astype(BF16)
            acc[rows, :] += dot_nt(jnp.concatenate([ds, probs.astype(BF16)], axis=1), m)
            total = total + dot(kt[:, 256 * c : 256 * c + 256], ds)
        dqp[slot] = total

    def dq_y(t, u, device):
        return copy(DQ_Y + 3 * t + u - 1, dqp.at[4 * t + u], dqr.at[3 * t + u - 1], device)

    def back(u):
        return dev(0, jnp.where(u == 1, -1, jnp.where(u == 2, 1, 2)))

    def steps(t, first):
        def step(u, carry):
            copy(Q_Y + 3 * t + u - 1, qbuf.at[4 * t], qbuf.at[4 * t + u], dev(0, 1)).wait_recv()
            process(4 * t + u)
            dq_y(t, u, back(u)).start()
            return carry

        if first:
            process(4 * t)
        lax.fori_loop(1, 4, step, 0)

    q_far[0].wait_recv()
    q_far[1].wait_recv()
    q_far[2].start()
    for t in (1, 2):
        for c in q_y[t]:
            c.start()
    steps(0, True)
    process(4)
    process(8)
    q_far[2].wait_recv()
    for c in q_y[3]:
        c.start()
    steps(1, False)
    steps(2, False)
    steps(3, True)

    lane_scale = jnp.where(lane < NOPE, SCALE, 1.0)
    for c in lat:
        c.wait_recv()
    wpart = jnp.zeros((RANK, 128), F32)
    dkv = []
    for s in (1, 2, 3, 0):
        main = acc[ROWS * s : ROWS * (s + 1), 0:128] * lane_scale
        dkvs[s] = main
        rots[s] = jnp.transpose(acc[ROWS * s : ROWS * (s + 1), 128:256])[0:ROPE] * SCALE
        if s:
            owner = dev(-k_off[s], 0)
            dkv.append(copy(DKV + s - 1, dkvs.at[s], dkvr.at[s - 1], owner))
            dkv.append(copy(DROT + s - 1, rots.at[s], rotr.at[s - 1], owner))
            dkv[-2].start()
            dkv[-1].start()
        hi = main.astype(BF16)
        low = (main - hi.astype(F32)).astype(BF16)
        wpart = wpart + dot(latt[s], hi) + dot(latt[s], low)
    wpart = wpart.reshape(NZ, NY, 8, 128)
    for v in range(NY):
        wsend[v] = wpart[:, v]
    w_y = []
    for u in (1, 2, 3):
        w_y.append(copy(W_Y + u - 1, wsend.at[(y + y_off[u] + NY) % NY], wrecv.at[u - 1], dev(0, y_off[u])))
        w_y[-1].start()

    def dq_sum(t):
        for u in (1, 2, 3):
            dq_y(t, u, dev(0, 1)).wait_recv()
        dqs[t] = dqp[4 * t] + dqr[3 * t] + dqr[3 * t + 1] + dqr[3 * t + 2]

    for t in (3, 1, 2, 0):
        dq_sum(t)
        if t == 3:
            dq_relay = copy(DQ_Z, dqs.at[3], dqz.at[0], dev(4 * sign, 0))
            dq_relay.start()
    dq_plain = copy(DQ_Z + 1, dqs.at[1 + odd], dqz.at[1], dev(-4 * sign, 0))
    dq_plain.start()

    for c in w_y:
        c.wait_recv()
    wzs[...] = wsend[y] + wrecv[0] + wrecv[1] + wrecv[2]
    w_z = []
    for d in range(1, NZ):
        w_z.append(copy(W_Z + d - 1, wzs.at[(z + d) % NZ], wzr.at[d - 1], dev(d, 0)))
        w_z[-1].start()

    for c in dkv:
        c.wait_recv()
    own = dkvs[0] + dkvr[0] + dkvr[1] + dkvr[2]
    rotx[tp] = rots[0] + rotr[0] + rotr[1] + rotr[2]
    rot = []
    for k in range(1, NTP):
        rot.append(copy(ROT + k - 1, rotx.at[tp], rotx.at[tp], (sp, (tp + k) % NTP)))
        rot[-1].start()
    own = own.astype(BF16)
    dk_ref[...] = own[:, 0:NOPE]
    dv_ref[...] = own[:, NOPE:128]

    dq_relay.wait_recv()
    dqs[2 - odd] = dqs[2 - odd] + dqz[0]
    dq_last = copy(DQ_Z + 2, dqs.at[2 - odd], dqz.at[2], dev(4 * sign, 0))
    dq_last.start()

    for k in range(1, NTP):
        rot[k - 1].wait_recv()
    total = rotx[0]
    for k in range(1, NTP):
        total = total + rotx[k]
    drot_ref[...] = jnp.transpose(jnp.concatenate([total, jnp.zeros((96, ROWS), F32)], axis=0))[:, 0:ROPE]

    for c in w_z:
        c.wait_recv()
    wsum = wzs[z]
    for d in range(1, NZ):
        wsum = wsum + wzr[d - 1]
    dw_ref[...] = wsum

    dq_plain.wait_recv()
    dq_last.wait_recv()
    dq_total = (dqs[0] + dqz[1] + dqz[2]) * SCALE
    dq_total = jnp.transpose(jnp.concatenate([dq_total, jnp.zeros((32, ROWS), F32)], axis=0))
    dq_ref[...] = dq_total[:, 0:96].astype(BF16)

    for c in q_far + kv + lat + dkv + w_y + w_z + rot + [dq_relay, dq_plain, dq_last]:
        c.wait_send()
    for t in range(4):
        for c in q_y[t]:
            c.wait_send()
        for u in (1, 2, 3):
            dq_y(t, u, dev(0, 1)).wait_send()


def per_device(*arrays):
    vmem = pl.BlockSpec(memory_space=pltpu.VMEM)
    shape = jax.ShapeDtypeStruct
    return pl.pallas_call(
        kernel,
        out_shape=(
            shape((ROWS, NOPE + ROPE), BF16),
            shape((ROWS, NOPE), BF16),
            shape((ROWS, VAL), BF16),
            shape((ROWS, ROPE), F32),
            shape((8, 128), F32),
        ),
        in_specs=[vmem] * 7,
        out_specs=(vmem,) * 5,
        scratch_shapes=[
            pltpu.VMEM((16, PACK, ROWS), BF16),
            pltpu.VMEM((4 * ROWS, 256), BF16),
            pltpu.VMEM((96, 4 * ROWS), BF16),
            pltpu.VMEM((4, RANK, ROWS), BF16),
            pltpu.VMEM((256, 256), BF16),
            pltpu.VMEM((4 * ROWS, 256), F32),
            pltpu.VMEM((16, 96, ROWS), F32),
            pltpu.VMEM((12, 96, ROWS), F32),
            pltpu.VMEM((4, 96, ROWS), F32),
            pltpu.VMEM((3, 96, ROWS), F32),
            pltpu.VMEM((4, ROWS, 128), F32),
            pltpu.VMEM((3, ROWS, 128), F32),
            pltpu.VMEM((4, ROPE, ROWS), F32),
            pltpu.VMEM((3, ROPE, ROWS), F32),
            pltpu.VMEM((NTP, ROPE, ROWS), F32),
            pltpu.VMEM((NY, NZ, 8, 128), F32),
            pltpu.VMEM((3, NZ, 8, 128), F32),
            pltpu.VMEM((NZ, 8, 128), F32),
            pltpu.VMEM((NZ - 1, 8, 128), F32),
            pltpu.SemaphoreType.DMA((COPIES,)),
            pltpu.SemaphoreType.DMA((COPIES,)),
        ],
        compiler_params=pltpu.CompilerParams(collective_id=0, has_side_effects=True),
    )(*arrays)


def solution(mesh):
    placed = (
        P("sp", "tp"),
        P("sp", None),
        P("sp", None),
        P(None, "tp"),
        P("sp", "tp"),
        P("sp", "tp"),
        P("sp", "tp"),
    )
    return jax.shard_map(
        per_device,
        mesh=mesh,
        in_specs=placed,
        out_specs=(P("sp", "tp"), P("sp", "tp"), P("sp", "tp"), P("sp", None), P("sp", "tp")),
        check_vma=False,
    )
```

```python
import jax
import jax.numpy as jnp
from jax import lax
from jax.experimental import pallas as pl
from jax.experimental.pallas import tpu as pltpu
from jax.sharding import PartitionSpec as P

MESH = pl.DeviceIdType.MESH
F32 = jnp.float32
BF16 = jnp.bfloat16

NOPE = 64
ROPE = 32
VAL = 64
RANK = 512
ROWS = 128
NY = 4
NZ = 16
NTP = 8
PACK = 176
SCALE = (NOPE + ROPE) ** -0.5
LOG2E = 1.4426950408889634

Q_FAR = 0
Q_Y = 3
KV = 15
LAT = 18
DQ_Y = 21
DQ_Z = 33
DKV = 36
DROT = 39
W_Y = 42
W_Z = 45
ROT = 60
COPIES = 67


def three(x):
    hi = x.astype(BF16)
    rest = x - hi.astype(F32)
    mid = rest.astype(BF16)
    low = (rest - mid.astype(F32)).astype(BF16)
    return [hi.astype(F32), mid.astype(F32), low.astype(F32)]


def dot(a, b):
    return jnp.dot(a, b, preferred_element_type=F32)


def dot_nt(a, b):
    return lax.dot_general(a, b, (((1,), (1,)), ((), ())), preferred_element_type=F32)


def kernel(
    q_ref, lat_ref, rot_ref, w_ref, lse_ref, o_ref, do_ref,
    dq_ref, dk_ref, dv_ref, drot_ref, dw_ref,
    qbuf, kvbuf, kt, latt, mbuf, acc, dqp, dqr, dqs, dqz, dkvs, dkvr, rots, rotr, rotx, wsend, wrecv, wzs, wzr,
    ssem, rsem,
):
    sp = lax.axis_index("sp")
    tp = lax.axis_index("tp")
    z = sp // NY
    y = sp % NY
    odd = z % 2
    sign = 1 - 2 * odd

    def dev(dz, dy):
        return (((z + dz + NZ) % NZ) * NY + (y + dy + NY) % NY, tp)

    y_off = (0, 1, -1, 2)
    k_off = (0, 1, -1, 2 * sign)

    def copy(number, src, dst, device):
        return pltpu.make_async_remote_copy(
            src_ref=src, dst_ref=dst, send_sem=ssem.at[number], recv_sem=rsem.at[number],
            device_id=device, device_id_type=MESH,
        )

    barrier = pltpu.get_barrier_semaphore()
    greet = [dev(d, 0) for d in (1, -1, 2, -2, 4, -4)] + [dev(0, d) for d in (1, -1, 2)]
    greet += [(sp, (tp + k) % NTP) for k in range(1, NTP)]
    for device in greet:
        pl.semaphore_signal(barrier, inc=1, device_id=device, device_id_type=MESH)

    delta = jnp.sum(o_ref[...].astype(F32) * do_ref[...].astype(F32), axis=0, keepdims=True)
    lse = lse_ref[...] * (1.0 / SCALE)
    row = lax.broadcasted_iota(jnp.int32, (16, ROWS), 0)
    aux = jnp.zeros((16, ROWS), F32)
    for i, piece in enumerate(three(lse) + three(delta)):
        aux = jnp.where(row == i, jnp.broadcast_to(piece, (16, ROWS)), aux)
    qbuf[0, 0:64, :] = q_ref[0:64, :]
    qbuf[0, 64:128, :] = do_ref[...]
    qbuf[0, 128:160, :] = q_ref[64:96, :]
    qbuf[0, 160:176, :] = aux.astype(BF16)

    pl.semaphore_wait(barrier, len(greet))

    q_far = [
        copy(Q_FAR + 0, qbuf.at[0], qbuf.at[8], dev(-4, 0)),
        copy(Q_FAR + 1, qbuf.at[0], qbuf.at[4], dev(4, 0)),
        copy(Q_FAR + 2, qbuf.at[4 + 4 * odd], qbuf.at[12], dev(4 * sign, 0)),
    ]
    q_far[0].start()
    q_far[1].start()
    q_y = [
        [copy(Q_Y + 3 * t + u - 1, qbuf.at[4 * t], qbuf.at[4 * t + u], dev(0, y_off[u])) for u in (1, 2, 3)]
        for t in range(4)
    ]
    for c in q_y[0]:
        c.start()

    joined = dot(lat_ref[...], w_ref[...]).astype(BF16)
    kvbuf[0:ROWS, 0:128] = joined
    lane = lax.broadcasted_iota(jnp.int32, (ROWS, 128), 1)
    rot_rows = jnp.concatenate([rot_ref[...].astype(F32), jnp.zeros((ROWS - ROPE, ROWS), F32)], axis=0)
    marks = jnp.where((lane >= ROPE) & (lane < ROPE + 6), -1.0, 0.0)
    kvbuf[0:ROWS, 128:256] = (jnp.transpose(rot_rows) + marks).astype(BF16)

    def rows_of(s):
        return pl.ds(ROWS * s, ROWS)

    kv = [copy(KV + s - 1, kvbuf.at[rows_of(0)], kvbuf.at[rows_of(s)], dev(k_off[s], 0)) for s in (1, 2, 3)]
    for c in kv:
        c.start()
    latt[0] = jnp.transpose(lat_ref[...].astype(F32)).astype(BF16)
    lat = [copy(LAT + s - 1, latt.at[0], latt.at[s], dev(k_off[s], 0)) for s in (1, 2, 3)]
    for c in lat:
        c.start()

    mbuf[...] = jnp.zeros_like(mbuf)
    acc[...] = jnp.zeros_like(acc)

    for c in kv:
        c.wait_recv()
    kt[0:64, :] = jnp.transpose(kvbuf[:, 0:128].astype(F32))[0:64].astype(BF16)
    kt[64:96, :] = jnp.transpose(kvbuf[:, 128:256].astype(F32))[0:32].astype(BF16)

    def process(slot):
        mbuf[0:64, 0:128] = qbuf[slot, 0:64, :]
        mbuf[64:128, 128:256] = qbuf[slot, 64:128, :]
        mbuf[128:160, 0:128] = qbuf[slot, 128:160, :]
        extra = qbuf[slot, 160:176, :].astype(F32)
        mbuf[160:176, 0:128] = jnp.where(row < 3, extra, 0.0).astype(BF16)
        mbuf[160:176, 128:256] = jnp.where(row >= 3, extra, 0.0).astype(BF16)
        m = mbuf[...]
        total = jnp.zeros((96, ROWS), F32)
        for c in range(2):
            rows = pl.ds(256 * c, 256)
            both = dot(kvbuf[rows, :], m)
            probs = jnp.exp2(both[:, 0:128] * (SCALE * LOG2E))
            ds = (probs * both[:, 128:256]).astype(BF16)
            acc[rows, :] += dot_nt(jnp.concatenate([ds, probs.astype(BF16)], axis=1), m)
            total = total + dot(kt[:, 256 * c : 256 * c + 256], ds)
        dqp[slot] = total

    def dq_y(t, u, device):
        return copy(DQ_Y + 3 * t + u - 1, dqp.at[4 * t + u], dqr.at[3 * t + u - 1], device)

    def back(u):
        return dev(0, jnp.where(u == 1, -1, jnp.where(u == 2, 1, 2)))

    def steps(t, first):
        def step(u, carry):
            copy(Q_Y + 3 * t + u - 1, qbuf.at[4 * t], qbuf.at[4 * t + u], dev(0, 1)).wait_recv()
            process(4 * t + u)
            dq_y(t, u, back(u)).start()
            return carry

        if first:
            process(4 * t)
        lax.fori_loop(1, 4, step, 0)

    q_far[0].wait_recv()
    q_far[1].wait_recv()
    q_far[2].start()
    for t in (1, 2):
        for c in q_y[t]:
            c.start()
    steps(0, True)
    process(4)
    process(8)
    q_far[2].wait_recv()
    for c in q_y[3]:
        c.start()
    steps(1, False)
    steps(2, False)
    steps(3, True)

    lane_scale = jnp.where(lane < NOPE, SCALE, 1.0)
    for c in lat:
        c.wait_recv()
    wpart = jnp.zeros((RANK, 128), F32)
    dkv = []
    for s in (1, 2, 3, 0):
        main = acc[ROWS * s : ROWS * (s + 1), 0:128] * lane_scale
        dkvs[s] = main
        rots[s] = jnp.transpose(acc[ROWS * s : ROWS * (s + 1), 128:256])[0:ROPE] * SCALE
        if s:
            owner = dev(-k_off[s], 0)
            dkv.append(copy(DKV + s - 1, dkvs.at[s], dkvr.at[s - 1], owner))
            dkv.append(copy(DROT + s - 1, rots.at[s], rotr.at[s - 1], owner))
            dkv[-2].start()
            dkv[-1].start()
        hi = main.astype(BF16)
        low = (main - hi.astype(F32)).astype(BF16)
        wpart = wpart + dot(latt[s], hi) + dot(latt[s], low)
    wpart = wpart.reshape(NZ, NY, 8, 128)
    for v in range(NY):
        wsend[v] = wpart[:, v]
    w_y = []
    for u in (1, 2, 3):
        w_y.append(copy(W_Y + u - 1, wsend.at[(y + y_off[u] + NY) % NY], wrecv.at[u - 1], dev(0, y_off[u])))
        w_y[-1].start()

    def dq_sum(t):
        for u in (1, 2, 3):
            dq_y(t, u, dev(0, 1)).wait_recv()
        dqs[t] = dqp[4 * t] + dqr[3 * t] + dqr[3 * t + 1] + dqr[3 * t + 2]

    for t in (3, 1, 2, 0):
        dq_sum(t)
        if t == 3:
            dq_relay = copy(DQ_Z, dqs.at[3], dqz.at[0], dev(4 * sign, 0))
            dq_relay.start()
    dq_plain = copy(DQ_Z + 1, dqs.at[1 + odd], dqz.at[1], dev(-4 * sign, 0))
    dq_plain.start()

    for c in w_y:
        c.wait_recv()
    wzs[...] = wsend[y] + wrecv[0] + wrecv[1] + wrecv[2]
    w_z = []
    for d in range(1, NZ):
        w_z.append(copy(W_Z + d - 1, wzs.at[(z + d) % NZ], wzr.at[d - 1], dev(d, 0)))
        w_z[-1].start()

    for c in dkv:
        c.wait_recv()
    own = dkvs[0] + dkvr[0] + dkvr[1] + dkvr[2]
    rotx[tp] = rots[0] + rotr[0] + rotr[1] + rotr[2]
    rot = []
    for k in range(1, NTP):
        rot.append(copy(ROT + k - 1, rotx.at[tp], rotx.at[tp], (sp, (tp + k) % NTP)))
        rot[-1].start()
    own = jnp.transpose(own).astype(BF16)
    dk_ref[...] = own[0:NOPE]
    dv_ref[...] = own[NOPE:128]

    dq_relay.wait_recv()
    dqs[2 - odd] = dqs[2 - odd] + dqz[0]
    dq_last = copy(DQ_Z + 2, dqs.at[2 - odd], dqz.at[2], dev(4 * sign, 0))
    dq_last.start()

    for k in range(1, NTP):
        rot[k - 1].wait_recv()
    total = rotx[0]
    for k in range(1, NTP):
        total = total + rotx[k]
    drot_ref[...] = total

    for c in w_z:
        c.wait_recv()
    wsum = wzs[z]
    for d in range(1, NZ):
        wsum = wsum + wzr[d - 1]
    dw_ref[...] = wsum

    dq_plain.wait_recv()
    dq_last.wait_recv()
    dq_ref[...] = ((dqs[0] + dqz[1] + dqz[2]) * SCALE).astype(BF16)

    for c in q_far + kv + lat + dkv + w_y + w_z + rot + [dq_relay, dq_plain, dq_last]:
        c.wait_send()
    for t in range(4):
        for c in q_y[t]:
            c.wait_send()
        for u in (1, 2, 3):
            dq_y(t, u, dev(0, 1)).wait_send()


def per_device(queries, latents, rot_key, kv_weight, log_sums, outputs, out_grad):
    vmem = pl.BlockSpec(memory_space=pltpu.VMEM)
    shape = jax.ShapeDtypeStruct
    dq, dk, dv, drot, dw = pl.pallas_call(
        kernel,
        out_shape=(
            shape((NOPE + ROPE, ROWS), BF16),
            shape((NOPE, ROWS), BF16),
            shape((VAL, ROWS), BF16),
            shape((ROPE, ROWS), F32),
            shape((8, 128), F32),
        ),
        in_specs=[vmem] * 7,
        out_specs=(vmem,) * 5,
        scratch_shapes=[
            pltpu.VMEM((16, PACK, ROWS), BF16),
            pltpu.VMEM((4 * ROWS, 256), BF16),
            pltpu.VMEM((96, 4 * ROWS), BF16),
            pltpu.VMEM((4, RANK, ROWS), BF16),
            pltpu.VMEM((256, 256), BF16),
            pltpu.VMEM((4 * ROWS, 256), F32),
            pltpu.VMEM((16, 96, ROWS), F32),
            pltpu.VMEM((12, 96, ROWS), F32),
            pltpu.VMEM((4, 96, ROWS), F32),
            pltpu.VMEM((3, 96, ROWS), F32),
            pltpu.VMEM((4, ROWS, 128), F32),
            pltpu.VMEM((3, ROWS, 128), F32),
            pltpu.VMEM((4, ROPE, ROWS), F32),
            pltpu.VMEM((3, ROPE, ROWS), F32),
            pltpu.VMEM((NTP, ROPE, ROWS), F32),
            pltpu.VMEM((NY, NZ, 8, 128), F32),
            pltpu.VMEM((3, NZ, 8, 128), F32),
            pltpu.VMEM((NZ, 8, 128), F32),
            pltpu.VMEM((NZ - 1, 8, 128), F32),
            pltpu.SemaphoreType.DMA((COPIES,)),
            pltpu.SemaphoreType.DMA((COPIES,)),
        ],
        compiler_params=pltpu.CompilerParams(collective_id=0, has_side_effects=True),
    )(queries.T, latents, rot_key.T, kv_weight, log_sums.T, outputs.T, out_grad.T)
    return dq.T, dk.T, dv.T, drot.T, dw


def solution(mesh):
    placed = (
        P("sp", "tp"),
        P("sp", None),
        P("sp", None),
        P(None, "tp"),
        P("sp", "tp"),
        P("sp", "tp"),
        P("sp", "tp"),
    )
    return jax.shard_map(
        per_device,
        mesh=mesh,
        in_specs=placed,
        out_specs=(P("sp", "tp"), P("sp", "tp"), P("sp", "tp"), P("sp", None), P("sp", "tp")),
        check_vma=False,
    )
```

```python
import jax
import jax.numpy as jnp
from jax import lax
from jax.experimental import pallas as pl
from jax.experimental.pallas import tpu as pltpu
from jax.sharding import PartitionSpec as P

MESH = pl.DeviceIdType.MESH
F32 = jnp.float32
BF16 = jnp.bfloat16

NOPE = 64
ROPE = 32
VAL = 64
RANK = 512
ROWS = 128
NY = 4
NZ = 16
NTP = 8
PART = RANK // NTP
PACK = 176
SCALE = (NOPE + ROPE) ** -0.5
LOG2E = 1.4426950408889634

Q_FAR = 0
Q_Y = 3
KV = 15
KROT = 18
LAT = 21
LAT_TP = 24
DQ_Y = 31
DQ_Z = 43
DKV = 46
DROT = 49
W_Y = 52
W_Z = 55
ROT = 70
COPIES = 77


def three(x):
    hi = x.astype(BF16)
    rest = x - hi.astype(F32)
    mid = rest.astype(BF16)
    low = (rest - mid.astype(F32)).astype(BF16)
    return [hi.astype(F32), mid.astype(F32), low.astype(F32)]


def dot(a, b):
    return jnp.dot(a, b, preferred_element_type=F32)


def dot_nt(a, b):
    return lax.dot_general(a, b, (((1,), (1,)), ((), ())), preferred_element_type=F32)


def kernel(
    q_hbm, lat_hbm, rot_hbm, w_hbm, lse_hbm, o_hbm, do_hbm,
    dq_ref, dk_ref, dv_ref, drot_ref, dw_ref,
    q_ref, lat_ref, w_ref, lse_ref, o_ref, do_ref,
    qbuf, kvm, kvx, krot, kt, latt, mbuf, acc, dqp, dqr, dqs, dqz, dkvs, dkvr, rots, rotr, rotx, wsend, wrecv, wzs, wzr,
    isem, ssem, rsem,
):
    sp = lax.axis_index("sp")
    tp = lax.axis_index("tp")
    z = sp // NY
    y = sp % NY
    sign = 1 - 2 * (z % 2)

    def dev(dz, dy):
        return (((z + dz + NZ) % NZ) * NY + (y + dy + NY) % NY, tp)

    y_off = (0, 1, -1, 2)
    k_off = (0, 1, -1, 2 * sign)

    def copy(number, src, dst, device):
        return pltpu.make_async_remote_copy(
            src_ref=src, dst_ref=dst, send_sem=ssem.at[number], recv_sem=rsem.at[number],
            device_id=device, device_id_type=MESH,
        )

    def others(k):
        return (sp, (tp + k) % NTP)

    loads = [
        pltpu.make_async_copy(src, dst, isem.at[i])
        for i, (src, dst) in enumerate((
            (o_hbm, o_ref), (do_hbm, do_ref), (q_hbm, q_ref), (lse_hbm, lse_ref),
            (lat_hbm, lat_ref), (w_hbm, w_ref), (rot_hbm, krot.at[0]),
        ))
    ]
    barrier = pltpu.get_barrier_semaphore()
    greet = [dev(d, 0) for d in (4, -4, 1, -1, 2, -2)] + [dev(0, d) for d in (1, -1, 2)]
    greet += [others(k) for k in range(1, NTP)]
    for device in greet:
        pl.semaphore_signal(barrier, inc=1, device_id=device, device_id_type=MESH)
    for c in loads:
        c.start()
    mbuf[...] = jnp.zeros_like(mbuf)
    acc[...] = jnp.zeros_like(acc)

    for c in loads[0:4]:
        c.wait()
    delta = jnp.sum(o_ref[...].astype(F32) * do_ref[...].astype(F32), axis=0, keepdims=True)
    lse = lse_ref[...] * (1.0 / SCALE)
    row = lax.broadcasted_iota(jnp.int32, (16, ROWS), 0)
    aux = jnp.zeros((16, ROWS), F32)
    for i, piece in enumerate(three(lse) + three(delta)):
        aux = jnp.where(row == i, jnp.broadcast_to(piece, (16, ROWS)), aux)
    qbuf[0, 0:64, :] = q_ref[0:64, :]
    qbuf[0, 64:128, :] = do_ref[...]
    qbuf[0, 128:160, :] = q_ref[64:96, :]
    qbuf[0, 160:176, :] = aux.astype(BF16)

    for c in loads[4:7]:
        c.wait()
    kvm[0:ROWS, :] = dot(lat_ref[...], w_ref[...]).astype(BF16)
    latt[0] = jnp.transpose(lat_ref[...].astype(F32)).astype(BF16)

    pl.semaphore_wait(barrier, len(greet))

    def rows_of(s):
        return pl.ds(ROWS * s, ROWS)

    q_far = [
        copy(Q_FAR + 0, qbuf.at[0], qbuf.at[4], dev(4 * sign, 0)),
        copy(Q_FAR + 1, qbuf.at[0], qbuf.at[8], dev(-4 * sign, 0)),
        copy(Q_FAR + 2, qbuf.at[4], qbuf.at[12], dev(4 * sign, 0)),
    ]
    q_y = [
        [copy(Q_Y + 3 * t + u - 1, qbuf.at[4 * t], qbuf.at[4 * t + u], dev(0, y_off[u])) for u in (1, 2, 3)]
        for t in range(4)
    ]
    mine = pl.ds(PART * tp, PART)
    kv = [copy(KV + s - 1, kvm.at[rows_of(0)], kvm.at[rows_of(s)], dev(k_off[s], 0)) for s in (1, 2, 3)]
    kv += [copy(KROT + s - 1, krot.at[0], krot.at[s], dev(k_off[s], 0)) for s in (1, 2, 3)]
    lat = [copy(LAT + s - 1, latt.at[0, mine], latt.at[s, mine], dev(k_off[s], 0)) for s in (1, 2, 3)]
    q_far[0].start()
    for c in kv:
        c.start()
    q_far[1].start()
    for c in q_y[0]:
        c.start()
    for c in lat:
        c.start()

    for c in kv:
        c.wait_recv()
    kt[0:64, :] = jnp.transpose(kvm[...].astype(F32))[0:64].astype(BF16)
    lane = lax.broadcasted_iota(jnp.int32, (ROWS, 128), 1)
    marks = jnp.where((lane >= ROPE) & (lane < ROPE + 6), -1.0, 0.0)
    for s in range(4):
        rot_rows = jnp.concatenate([krot[s].astype(F32), jnp.zeros((ROWS - ROPE, ROWS), F32)], axis=0)
        kvx[ROWS * s : ROWS * (s + 1), :] = (jnp.transpose(rot_rows) + marks).astype(BF16)
        kt[64:96, ROWS * s : ROWS * (s + 1)] = krot[s]

    def process(slot):
        mbuf[0:64, 0:128] = qbuf[slot, 0:64, :]
        mbuf[64:128, 128:256] = qbuf[slot, 64:128, :]
        mbuf[128:160, 0:128] = qbuf[slot, 128:160, :]
        extra = qbuf[slot, 160:176, :].astype(F32)
        mbuf[160:176, 0:128] = jnp.where(row < 3, extra, 0.0).astype(BF16)
        mbuf[160:176, 128:256] = jnp.where(row >= 3, extra, 0.0).astype(BF16)
        m = mbuf[...]
        total = jnp.zeros((96, ROWS), F32)
        for c in range(2):
            rows = pl.ds(256 * c, 256)
            both = dot(jnp.concatenate([kvm[rows, :], kvx[rows, :]], axis=1), m)
            probs = jnp.exp2(both[:, 0:128] * (SCALE * LOG2E))
            ds = (probs * both[:, 128:256]).astype(BF16)
            acc[rows, :] += dot_nt(jnp.concatenate([ds, probs.astype(BF16)], axis=1), m)
            total = total + dot(kt[:, 256 * c : 256 * c + 256], ds)
        dqp[slot] = total

    def dq_y(t, u, device):
        return copy(DQ_Y + 3 * t + u - 1, dqp.at[4 * t + u], dqr.at[3 * t + u - 1], device)

    def back(u):
        return dev(0, jnp.where(u == 1, -1, jnp.where(u == 2, 1, 2)))

    def steps(t, first):
        def step(u, carry):
            copy(Q_Y + 3 * t + u - 1, qbuf.at[4 * t], qbuf.at[4 * t + u], dev(0, 1)).wait_recv()
            process(4 * t + u)
            dq_y(t, u, back(u)).start()
            return carry

        if first:
            process(4 * t)
        lax.fori_loop(1, 4, step, 0)

    q_far[0].wait_recv()
    q_far[2].start()
    for c in q_y[1]:
        c.start()
    q_far[1].wait_recv()
    for c in q_y[2]:
        c.start()
    for c in lat:
        c.wait_recv()
    lat_tp = [
        copy(LAT_TP + k - 1, latt.at[pl.ds(1, 3), mine], latt.at[pl.ds(1, 3), mine], others(k)) for k in range(1, NTP)
    ]
    for c in lat_tp:
        c.start()
    steps(0, True)
    process(4)
    process(8)
    q_far[2].wait_recv()
    for c in q_y[3]:
        c.start()
    steps(1, False)
    steps(2, False)
    steps(3, True)

    lane_scale = jnp.where(lane < NOPE, SCALE, 1.0)
    for c in lat_tp:
        c.wait_recv()
    wpart = jnp.zeros((RANK, 128), F32)
    dkv = []
    for s in (1, 2, 3, 0):
        main = acc[ROWS * s : ROWS * (s + 1), 0:128] * lane_scale
        dkvs[s] = main
        rots[s] = jnp.transpose(acc[ROWS * s : ROWS * (s + 1), 128:256])[0:ROPE] * SCALE
        if s:
            owner = dev(-k_off[s], 0)
            dkv.append(copy(DKV + s - 1, dkvs.at[s], dkvr.at[s - 1], owner))
            dkv.append(copy(DROT + s - 1, rots.at[s], rotr.at[s - 1], owner))
            dkv[-2].start()
            dkv[-1].start()
        hi = main.astype(BF16)
        low = (main - hi.astype(F32)).astype(BF16)
        wpart = wpart + dot(latt[s], hi) + dot(latt[s], low)
    wpart = wpart.reshape(NZ, NY, 8, 128)
    for v in range(NY):
        wsend[v] = wpart[:, v]
    w_y = []
    for u in (1, 2, 3):
        w_y.append(copy(W_Y + u - 1, wsend.at[(y + y_off[u] + NY) % NY], wrecv.at[u - 1], dev(0, y_off[u])))
        w_y[-1].start()

    dq_z = []
    for t, dz in ((1, -4 * sign), (2, 4 * sign), (3, 8), (0, 0)):
        for u in (1, 2, 3):
            dq_y(t, u, dev(0, 1)).wait_recv()
        dqs[t] = dqp[4 * t] + dqr[3 * t] + dqr[3 * t + 1] + dqr[3 * t + 2]
        if t:
            dq_z.append(copy(DQ_Z + t - 1, dqs.at[t], dqz.at[t - 1], dev(dz, 0)))
            dq_z[-1].start()

    for c in w_y:
        c.wait_recv()
    wzs[...] = wsend[y] + wrecv[0] + wrecv[1] + wrecv[2]
    w_z = []
    for d in (8, 7, 9, 6, 10, 5, 11, 4, 12, 3, 13, 2, 14, 1, 15):
        w_z.append(copy(W_Z + d - 1, wzs.at[(z + d) % NZ], wzr.at[d - 1], dev(d, 0)))
        w_z[-1].start()

    for c in dkv:
        c.wait_recv()
    own = dkvs[0] + dkvr[0] + dkvr[1] + dkvr[2]
    rotx[tp] = rots[0] + rotr[0] + rotr[1] + rotr[2]
    rot = []
    for k in range(1, NTP):
        rot.append(copy(ROT + k - 1, rotx.at[tp], rotx.at[tp], others(k)))
        rot[-1].start()
    own = jnp.transpose(own).astype(BF16)
    dk_ref[...] = own[0:NOPE]
    dv_ref[...] = own[NOPE:128]

    for c in rot:
        c.wait_recv()
    total = rotx[0]
    for k in range(1, NTP):
        total = total + rotx[k]
    drot_ref[...] = total

    for c in w_z:
        c.wait_recv()
    wsum = wzs[z]
    for d in range(1, NZ):
        wsum = wsum + wzr[d - 1]
    dw_ref[...] = wsum

    for c in dq_z:
        c.wait_recv()
    dq_ref[...] = ((dqs[0] + dqz[0] + dqz[1] + dqz[2]) * SCALE).astype(BF16)

    for c in q_far + kv + lat + lat_tp + dkv + w_y + w_z + rot + dq_z:
        c.wait_send()
    for t in range(4):
        for c in q_y[t]:
            c.wait_send()
        for u in (1, 2, 3):
            dq_y(t, u, dev(0, 1)).wait_send()


def hand_over(*refs):
    for src, dst in zip(refs[:5], refs[5:]):
        dst[...] = src[...]


def per_device(queries, latents, rot_key, kv_weight, log_sums, outputs, out_grad):
    vmem = pl.BlockSpec(memory_space=pltpu.VMEM)
    shape = jax.ShapeDtypeStruct
    results = (
        shape((NOPE + ROPE, ROWS), BF16),
        shape((NOPE, ROWS), BF16),
        shape((VAL, ROWS), BF16),
        shape((ROPE, ROWS), F32),
        shape((8, 128), F32),
    )
    made = pl.pallas_call(
        kernel,
        out_shape=results,
        in_specs=[pl.BlockSpec(memory_space=pl.ANY)] * 7,
        out_specs=(vmem,) * 5,
        scratch_shapes=[
            pltpu.VMEM((NOPE + ROPE, ROWS), BF16),
            pltpu.VMEM((ROWS, RANK), BF16),
            pltpu.VMEM((RANK, 128), BF16),
            pltpu.VMEM((1, ROWS), F32),
            pltpu.VMEM((VAL, ROWS), BF16),
            pltpu.VMEM((VAL, ROWS), BF16),
            pltpu.VMEM((16, PACK, ROWS), BF16),
            pltpu.VMEM((4 * ROWS, 128), BF16),
            pltpu.VMEM((4 * ROWS, 128), BF16),
            pltpu.VMEM((4, ROPE, ROWS), BF16),
            pltpu.VMEM((96, 4 * ROWS), BF16),
            pltpu.VMEM((4, RANK, ROWS), BF16),
            pltpu.VMEM((256, 256), BF16),
            pltpu.VMEM((4 * ROWS, 256), F32),
            pltpu.VMEM((16, 96, ROWS), F32),
            pltpu.VMEM((12, 96, ROWS), F32),
            pltpu.VMEM((4, 96, ROWS), F32),
            pltpu.VMEM((3, 96, ROWS), F32),
            pltpu.VMEM((4, ROWS, 128), F32),
            pltpu.VMEM((3, ROWS, 128), F32),
            pltpu.VMEM((4, ROPE, ROWS), F32),
            pltpu.VMEM((3, ROPE, ROWS), F32),
            pltpu.VMEM((NTP, ROPE, ROWS), F32),
            pltpu.VMEM((NY, NZ, 8, 128), F32),
            pltpu.VMEM((3, NZ, 8, 128), F32),
            pltpu.VMEM((NZ, 8, 128), F32),
            pltpu.VMEM((NZ - 1, 8, 128), F32),
            pltpu.SemaphoreType.DMA((7,)),
            pltpu.SemaphoreType.DMA((COPIES,)),
            pltpu.SemaphoreType.DMA((COPIES,)),
        ],
        compiler_params=pltpu.CompilerParams(collective_id=0, has_side_effects=True),
    )(queries.T, latents, rot_key.T, kv_weight, log_sums.T, outputs.T, out_grad.T)
    dq, dk, dv, drot, dw = pl.pallas_call(
        hand_over, out_shape=results, in_specs=[vmem] * 5, out_specs=(vmem,) * 5
    )(*made)
    return dq.T, dk.T, dv.T, drot.T, dw


def solution(mesh):
    placed = (
        P("sp", "tp"),
        P("sp", None),
        P("sp", None),
        P(None, "tp"),
        P("sp", "tp"),
        P("sp", "tp"),
        P("sp", "tp"),
    )
    return jax.shard_map(
        per_device,
        mesh=mesh,
        in_specs=placed,
        out_specs=(P("sp", "tp"), P("sp", "tp"), P("sp", "tp"), P("sp", None), P("sp", "tp")),
        check_vma=False,
    )
```

```python
import jax
import jax.numpy as jnp
from jax import lax
from jax.experimental import pallas as pl
from jax.experimental.pallas import tpu as pltpu
from jax.sharding import PartitionSpec as P

MESH = pl.DeviceIdType.MESH
F32 = jnp.float32
BF16 = jnp.bfloat16

NOPE = 64
ROPE = 32
VAL = 64
RANK = 512
ROWS = 128
NY = 4
NZ = 16
NTP = 8
PART = RANK // NTP
PACK = 176
SCALE = (NOPE + ROPE) ** -0.5
LOG2E = 1.4426950408889634

Q_FAR = 0
Q_Y = 3
KV = 15
KROT = 18
LAT = 21
LAT_TP = 24
DQ_Y = 31
DQ_Z = 43
DKV = 46
DROT = 49
W_Y = 52
W_Z = 55
ROT = 70
COPIES = 77


def three(x):
    hi = x.astype(BF16)
    rest = x - hi.astype(F32)
    mid = rest.astype(BF16)
    low = (rest - mid.astype(F32)).astype(BF16)
    return [hi.astype(F32), mid.astype(F32), low.astype(F32)]


def dot(a, b):
    return jnp.dot(a, b, preferred_element_type=F32)


def dot_nt(a, b):
    return lax.dot_general(a, b, (((1,), (1,)), ((), ())), preferred_element_type=F32)


def kernel(
    q_hbm, lat_hbm, rot_hbm, w_hbm, lse_hbm, o_hbm, do_hbm,
    dq_ref, dk_ref, dv_ref, drot_ref, dw_ref,
    q_ref, lat_ref, w_ref, lse_ref, o_ref, do_ref,
    qbuf, kvm, kvx, krot, kt, latt, mbuf, acc, dqp, dqr, dqs, dqz, dkvs, dkvr, halves, rots, rotr, rotx, wsend, wrecv, wzs, wzr,
    isem, ssem, rsem,
):
    sp = lax.axis_index("sp")
    tp = lax.axis_index("tp")
    z = sp // NY
    y = sp % NY
    sign = 1 - 2 * (z % 2)

    def dev(dz, dy):
        return (((z + dz + NZ) % NZ) * NY + (y + dy + NY) % NY, tp)

    y_off = (0, 1, -1, 2)
    k_off = (0, 1, -1, 2 * sign)

    def copy(number, src, dst, device):
        return pltpu.make_async_remote_copy(
            src_ref=src, dst_ref=dst, send_sem=ssem.at[number], recv_sem=rsem.at[number],
            device_id=device, device_id_type=MESH,
        )

    def others(k):
        return (sp, (tp + k) % NTP)

    loads = [
        pltpu.make_async_copy(src, dst, isem.at[i])
        for i, (src, dst) in enumerate((
            (o_hbm, o_ref), (do_hbm, do_ref), (q_hbm, q_ref), (lse_hbm, lse_ref),
            (lat_hbm, lat_ref), (w_hbm, w_ref), (rot_hbm, krot.at[0]),
        ))
    ]
    barrier = pltpu.get_barrier_semaphore()
    greet = [dev(d, 0) for d in (4, -4, 1, -1, 2, -2)] + [dev(0, d) for d in (1, -1, 2)]
    greet += [others(k) for k in range(1, NTP)]
    for device in greet:
        pl.semaphore_signal(barrier, inc=1, device_id=device, device_id_type=MESH)
    for c in loads:
        c.start()
    mbuf[...] = jnp.zeros_like(mbuf)
    acc[...] = jnp.zeros_like(acc)

    for c in loads[0:4]:
        c.wait()
    delta = jnp.sum(o_ref[...].astype(F32) * do_ref[...].astype(F32), axis=0, keepdims=True)
    lse = lse_ref[...] * (1.0 / SCALE)
    row = lax.broadcasted_iota(jnp.int32, (16, ROWS), 0)
    aux = jnp.zeros((16, ROWS), F32)
    for i, piece in enumerate(three(lse) + three(delta)):
        aux = jnp.where(row == i, jnp.broadcast_to(piece, (16, ROWS)), aux)
    qbuf[0, 0:64, :] = q_ref[0:64, :]
    qbuf[0, 64:128, :] = do_ref[...]
    qbuf[0, 128:160, :] = q_ref[64:96, :]
    qbuf[0, 160:176, :] = aux.astype(BF16)

    for c in loads[4:7]:
        c.wait()
    kvm[0:ROWS, :] = dot(lat_ref[...], w_ref[...]).astype(BF16)
    latt[0] = jnp.transpose(lat_ref[...].astype(F32)).astype(BF16)

    pl.semaphore_wait(barrier, len(greet))

    def rows_of(s):
        return pl.ds(ROWS * s, ROWS)

    q_far = [
        copy(Q_FAR + 0, qbuf.at[0], qbuf.at[4], dev(4 * sign, 0)),
        copy(Q_FAR + 1, qbuf.at[0], qbuf.at[8], dev(-4 * sign, 0)),
        copy(Q_FAR + 2, qbuf.at[4], qbuf.at[12], dev(4 * sign, 0)),
    ]
    q_y = [
        [copy(Q_Y + 3 * t + u - 1, qbuf.at[4 * t], qbuf.at[4 * t + u], dev(0, y_off[u])) for u in (1, 2, 3)]
        for t in range(4)
    ]
    mine = pl.ds(PART * tp, PART)
    kv = [copy(KV + s - 1, kvm.at[rows_of(0)], kvm.at[rows_of(s)], dev(k_off[s], 0)) for s in (1, 2, 3)]
    kv += [copy(KROT + s - 1, krot.at[0], krot.at[s], dev(k_off[s], 0)) for s in (1, 2, 3)]
    lat = [copy(LAT + s - 1, latt.at[0, mine], latt.at[s, mine], dev(k_off[s], 0)) for s in (1, 2, 3)]
    q_far[0].start()
    for c in kv:
        c.start()
    q_far[1].start()
    for c in q_y[0]:
        c.start()
    for c in lat:
        c.start()

    for c in kv:
        c.wait_recv()
    kt[0:64, :] = jnp.transpose(kvm[...].astype(F32))[0:64].astype(BF16)
    lane = lax.broadcasted_iota(jnp.int32, (ROWS, 128), 1)
    marks = jnp.where((lane >= ROPE) & (lane < ROPE + 6), -1.0, 0.0)
    for s in range(4):
        rot_rows = jnp.concatenate([krot[s].astype(F32), jnp.zeros((ROWS - ROPE, ROWS), F32)], axis=0)
        kvx[ROWS * s : ROWS * (s + 1), :] = (jnp.transpose(rot_rows) + marks).astype(BF16)
        kt[64:96, ROWS * s : ROWS * (s + 1)] = krot[s]

    def process(slot):
        mbuf[0:64, 0:128] = qbuf[slot, 0:64, :]
        mbuf[64:128, 128:256] = qbuf[slot, 64:128, :]
        mbuf[128:160, 0:128] = qbuf[slot, 128:160, :]
        extra = qbuf[slot, 160:176, :].astype(F32)
        mbuf[160:176, 0:128] = jnp.where(row < 3, extra, 0.0).astype(BF16)
        mbuf[160:176, 128:256] = jnp.where(row >= 3, extra, 0.0).astype(BF16)
        m = mbuf[...]
        total = jnp.zeros((96, ROWS), F32)
        for c in range(2):
            rows = pl.ds(256 * c, 256)
            both = dot(jnp.concatenate([kvm[rows, :], kvx[rows, :]], axis=1), m)
            probs = jnp.exp2(both[:, 0:128] * (SCALE * LOG2E))
            ds = (probs * both[:, 128:256]).astype(BF16)
            acc[rows, :] += dot_nt(jnp.concatenate([ds, probs.astype(BF16)], axis=1), m)
            total = total + dot(kt[:, 256 * c : 256 * c + 256], ds)
        dqp[slot] = total

    def dq_y(t, u, device):
        return copy(DQ_Y + 3 * t + u - 1, dqp.at[4 * t + u], dqr.at[3 * t + u - 1], device)

    def back(u):
        return dev(0, jnp.where(u == 1, -1, jnp.where(u == 2, 1, 2)))

    def steps(t):
        def step(u, carry):
            copy(Q_Y + 3 * t + u - 1, qbuf.at[4 * t], qbuf.at[4 * t + u], dev(0, 1)).wait_recv()
            process(4 * t + u)
            dq_y(t, u, back(u)).start()
            return carry

        lax.fori_loop(1, 4, step, 0)

    q_far[0].wait_recv()
    q_far[2].start()
    for c in q_y[1]:
        c.start()
    q_far[1].wait_recv()
    for c in q_y[2]:
        c.start()
    for c in lat:
        c.wait_recv()
    lat_tp = [
        copy(LAT_TP + k - 1, latt.at[pl.ds(1, 3), mine], latt.at[pl.ds(1, 3), mine], others(k)) for k in range(1, NTP)
    ]
    for c in lat_tp:
        c.start()
    process(0)
    steps(0)
    process(4)
    process(8)
    steps(1)
    steps(2)
    q_far[2].wait_recv()
    for c in q_y[3]:
        c.start()
    process(12)

    def dq_sum(t):
        for u in (1, 2, 3):
            dq_y(t, u, dev(0, 1)).wait_recv()
        return dqp[4 * t] + dqr[3 * t] + dqr[3 * t + 1] + dqr[3 * t + 2]

    dq_z = []

    def dq_send(t, dz):
        dqs[t - 1] = dq_sum(t).astype(BF16)
        dq_z.append(copy(DQ_Z + t - 1, dqs.at[t - 1], dqz.at[t - 1], dev(dz, 0)))
        dq_z[-1].start()

    dq_send(1, -4 * sign)
    dq_send(2, 4 * sign)
    steps(3)

    lane_scale = jnp.where(lane < NOPE, SCALE, 1.0)
    dkv = []
    for s in (1, 2, 3, 0):
        main = acc[ROWS * s : ROWS * (s + 1), 0:128] * lane_scale
        hi = main.astype(BF16)
        halves[ROWS * s : ROWS * (s + 1), 0:128] = hi
        halves[ROWS * s : ROWS * (s + 1), 128:256] = (main - hi.astype(F32)).astype(BF16)
        rots[s] = jnp.transpose(acc[ROWS * s : ROWS * (s + 1), 128:256])[0:ROPE] * SCALE
        if s:
            dkvs[s - 1] = hi
            owner = dev(-k_off[s], 0)
            dkv.append(copy(DKV + s - 1, dkvs.at[s - 1], dkvr.at[s - 1], owner))
            dkv.append(copy(DROT + s - 1, rots.at[s], rotr.at[s - 1], owner))
            dkv[-2].start()
            dkv[-1].start()
    for c in lat_tp:
        c.wait_recv()
    lat_all = jnp.concatenate([latt[0], latt[1], latt[2], latt[3]], axis=1)
    wpart = dot(lat_all, halves[...])
    wpart = (wpart[:, 0:128] + wpart[:, 128:256]).reshape(NZ, NY, 8, 128)
    for v in range(NY):
        wsend[v] = wpart[:, v]
    w_y = []
    for u in (1, 2, 3):
        w_y.append(copy(W_Y + u - 1, wsend.at[(y + y_off[u] + NY) % NY], wrecv.at[u - 1], dev(0, y_off[u])))
        w_y[-1].start()

    dq_send(3, 8)

    for c in w_y:
        c.wait_recv()
    wzs[...] = wsend[y] + wrecv[0] + wrecv[1] + wrecv[2]
    w_z = []
    for d in (8, 7, 9, 6, 10, 5, 11, 4, 12, 3, 13, 2, 14, 1, 15):
        w_z.append(copy(W_Z + d - 1, wzs.at[(z + d) % NZ], wzr.at[d - 1], dev(d, 0)))
        w_z[-1].start()

    for c in dkv:
        c.wait_recv()
    own = acc[0:ROWS, 0:128] * lane_scale
    for s in range(3):
        own = own + dkvr[s].astype(F32)
    rotx[tp] = rots[0] + rotr[0] + rotr[1] + rotr[2]
    rot = []
    for k in range(1, NTP):
        rot.append(copy(ROT + k - 1, rotx.at[tp], rotx.at[tp], others(k)))
        rot[-1].start()
    own = jnp.transpose(own).astype(BF16)
    dk_ref[...] = own[0:NOPE]
    dv_ref[...] = own[NOPE:128]

    for c in rot:
        c.wait_recv()
    total = rotx[0]
    for k in range(1, NTP):
        total = total + rotx[k]
    drot_ref[...] = total

    for c in w_z:
        c.wait_recv()
    wsum = wzs[z]
    for d in range(1, NZ):
        wsum = wsum + wzr[d - 1]
    dw_ref[...] = wsum

    total = dq_sum(0)
    for c in dq_z:
        c.wait_recv()
    for t in range(3):
        total = total + dqz[t].astype(F32)
    dq_ref[...] = (total * SCALE).astype(BF16)

    for c in q_far + kv + lat + lat_tp + dkv + w_y + w_z + rot + dq_z:
        c.wait_send()
    for t in range(4):
        for c in q_y[t]:
            c.wait_send()
        for u in (1, 2, 3):
            dq_y(t, u, dev(0, 1)).wait_send()


def hand_over(*refs):
    for src, dst in zip(refs[:5], refs[5:]):
        dst[...] = src[...]


def per_device(queries, latents, rot_key, kv_weight, log_sums, outputs, out_grad):
    vmem = pl.BlockSpec(memory_space=pltpu.VMEM)
    shape = jax.ShapeDtypeStruct
    results = (
        shape((NOPE + ROPE, ROWS), BF16),
        shape((NOPE, ROWS), BF16),
        shape((VAL, ROWS), BF16),
        shape((ROPE, ROWS), F32),
        shape((8, 128), F32),
    )
    made = pl.pallas_call(
        kernel,
        out_shape=results,
        in_specs=[pl.BlockSpec(memory_space=pl.ANY)] * 7,
        out_specs=(vmem,) * 5,
        scratch_shapes=[
            pltpu.VMEM((NOPE + ROPE, ROWS), BF16),
            pltpu.VMEM((ROWS, RANK), BF16),
            pltpu.VMEM((RANK, 128), BF16),
            pltpu.VMEM((1, ROWS), F32),
            pltpu.VMEM((VAL, ROWS), BF16),
            pltpu.VMEM((VAL, ROWS), BF16),
            pltpu.VMEM((16, PACK, ROWS), BF16),
            pltpu.VMEM((4 * ROWS, 128), BF16),
            pltpu.VMEM((4 * ROWS, 128), BF16),
            pltpu.VMEM((4, ROPE, ROWS), BF16),
            pltpu.VMEM((96, 4 * ROWS), BF16),
            pltpu.VMEM((4, RANK, ROWS), BF16),
            pltpu.VMEM((256, 256), BF16),
            pltpu.VMEM((4 * ROWS, 256), F32),
            pltpu.VMEM((16, 96, ROWS), F32),
            pltpu.VMEM((12, 96, ROWS), F32),
            pltpu.VMEM((3, 96, ROWS), BF16),
            pltpu.VMEM((3, 96, ROWS), BF16),
            pltpu.VMEM((3, ROWS, 128), BF16),
            pltpu.VMEM((3, ROWS, 128), BF16),
            pltpu.VMEM((4 * ROWS, 256), BF16),
            pltpu.VMEM((4, ROPE, ROWS), F32),
            pltpu.VMEM((3, ROPE, ROWS), F32),
            pltpu.VMEM((NTP, ROPE, ROWS), F32),
            pltpu.VMEM((NY, NZ, 8, 128), F32),
            pltpu.VMEM((3, NZ, 8, 128), F32),
            pltpu.VMEM((NZ, 8, 128), F32),
            pltpu.VMEM((NZ - 1, 8, 128), F32),
            pltpu.SemaphoreType.DMA((7,)),
            pltpu.SemaphoreType.DMA((COPIES,)),
            pltpu.SemaphoreType.DMA((COPIES,)),
        ],
        compiler_params=pltpu.CompilerParams(collective_id=0, has_side_effects=True),
    )(queries.T, latents, rot_key.T, kv_weight, log_sums.T, outputs.T, out_grad.T)
    dq, dk, dv, drot, dw = pl.pallas_call(
        hand_over, out_shape=results, in_specs=[vmem] * 5, out_specs=(vmem,) * 5
    )(*made)
    return dq.T, dk.T, dv.T, drot.T, dw


def solution(mesh):
    placed = (
        P("sp", "tp"),
        P("sp", None),
        P("sp", None),
        P(None, "tp"),
        P("sp", "tp"),
        P("sp", "tp"),
        P("sp", "tp"),
    )
    return jax.shard_map(
        per_device,
        mesh=mesh,
        in_specs=placed,
        out_specs=(P("sp", "tp"), P("sp", "tp"), P("sp", "tp"), P("sp", None), P("sp", "tp")),
        check_vma=False,
    )
```

```python
import jax
import jax.numpy as jnp
from jax import lax
from jax.experimental import pallas as pl
from jax.experimental.pallas import tpu as pltpu
from jax.sharding import PartitionSpec as P

MESH = pl.DeviceIdType.MESH
F32 = jnp.float32
BF16 = jnp.bfloat16

NOPE = 64
ROPE = 32
VAL = 64
RANK = 512
ROWS = 128
NY = 4
NZ = 16
NTP = 8
PART = RANK // NTP
PACK = 176
SCALE = (NOPE + ROPE) ** -0.5
LOG2E = 1.4426950408889634

K_FAR = 0
K_ROT = 3
LAT = 6
LAT_TP = 9
Q_N = 23
Q_Y = 26
DQ_Y = 38
DQ_N = 50
DKV = 53
DROT = 56
W_Y = 59
W_Z = 62
ROT = 77
COPIES = 84


def three(x):
    hi = x.astype(BF16)
    rest = x - hi.astype(F32)
    mid = rest.astype(BF16)
    low = (rest - mid.astype(F32)).astype(BF16)
    return [hi.astype(F32), mid.astype(F32), low.astype(F32)]


def dot(a, b):
    return jnp.dot(a, b, preferred_element_type=F32)


def dot_nt(a, b):
    return lax.dot_general(a, b, (((1,), (1,)), ((), ())), preferred_element_type=F32)


def kernel(
    q_hbm, lat_hbm, rot_hbm, w_hbm, lse_hbm, o_hbm, do_hbm,
    dq_ref, dk_ref, dv_ref, drot_ref, dw_ref,
    q_ref, lat_ref, w_ref, lse_ref, o_ref, do_ref,
    qbuf, kvm, kvx, krot, kt, latt, mall, acc, dqp, dqb, dqr, dqs, dqz, dkvs, dkvr, halves, rots, rotr, rotx,
    wsend, wrecv, wzs, wzr,
    isem, ssem, rsem,
):
    sp = lax.axis_index("sp")
    tp = lax.axis_index("tp")
    z = sp // NY
    y = sp % NY
    sign = 1 - 2 * (z % 2)

    def dev(dz, dy):
        return (((z + dz + NZ) % NZ) * NY + (y + dy + NY) % NY, tp)

    y_off = (0, 1, -1, 2)
    n_off = (0, 1, -1, 2 * sign)
    f_off = (0, 4 * sign, -4 * sign, 8)

    def copy(number, src, dst, device):
        return pltpu.make_async_remote_copy(
            src_ref=src, dst_ref=dst, send_sem=ssem.at[number], recv_sem=rsem.at[number],
            device_id=device, device_id_type=MESH,
        )

    def others(k):
        return (sp, (tp + k) % NTP)

    def rows_of(t):
        return pl.ds(ROWS * t, ROWS)

    loads = [
        pltpu.make_async_copy(src, dst, isem.at[i])
        for i, (src, dst) in enumerate((
            (lat_hbm, lat_ref), (w_hbm, w_ref), (rot_hbm, krot.at[0]),
            (o_hbm, o_ref), (do_hbm, do_ref), (q_hbm, q_ref), (lse_hbm, lse_ref),
        ))
    ]
    barrier = pltpu.get_barrier_semaphore()
    greet = [dev(d, 0) for d in (4, -4, 1, -1, 2, -2)] + [dev(0, d) for d in (1, -1, 2)]
    greet += [others(k) for k in range(1, NTP)]
    for device in greet:
        pl.semaphore_signal(barrier, inc=1, device_id=device, device_id_type=MESH)
    for c in loads:
        c.start()
    mall[...] = jnp.zeros_like(mall)
    acc[...] = jnp.zeros_like(acc)

    for c in loads[0:3]:
        c.wait()
    kvm[0:ROWS, :] = dot(lat_ref[...], w_ref[...]).astype(BF16)
    latt[0] = jnp.transpose(lat_ref[...].astype(F32)).astype(BF16)

    for c in loads[3:7]:
        c.wait()
    delta = jnp.sum(o_ref[...].astype(F32) * do_ref[...].astype(F32), axis=0, keepdims=True)
    lse = lse_ref[...] * (1.0 / SCALE)
    row = lax.broadcasted_iota(jnp.int32, (16, ROWS), 0)
    aux = jnp.zeros((16, ROWS), F32)
    for i, piece in enumerate(three(lse) + three(delta)):
        aux = jnp.where(row == i, jnp.broadcast_to(piece, (16, ROWS)), aux)
    qbuf[0, 0:64, :] = q_ref[0:64, :]
    qbuf[0, 64:128, :] = do_ref[...]
    qbuf[0, 128:160, :] = q_ref[64:96, :]
    qbuf[0, 160:176, :] = aux.astype(BF16)

    pl.semaphore_wait(barrier, len(greet))

    mine = pl.ds(PART * tp, PART)
    far = [
        [
            copy(K_FAR + t - 1, kvm.at[rows_of(a)], kvm.at[rows_of(t)], device),
            copy(K_ROT + t - 1, krot.at[a], krot.at[t], device),
            copy(LAT + t - 1, latt.at[a, mine], latt.at[t, mine], device),
        ]
        for t, a, device in ((1, 0, dev(4 * sign, 0)), (2, 0, dev(-4 * sign, 0)), (3, 1, dev(4 * sign, 0)))
    ]
    q_n = [copy(Q_N + s - 1, qbuf.at[0], qbuf.at[4 * s], dev(n_off[s], 0)) for s in (1, 2, 3)]
    q_y = [
        [copy(Q_Y + 3 * s + u - 1, qbuf.at[4 * s], qbuf.at[4 * s + u], dev(0, y_off[u])) for u in (1, 2, 3)]
        for s in range(4)
    ]
    for c in far[0] + q_n + far[1] + q_y[0]:
        c.start()
    for s in (1, 2, 3):
        q_n[s - 1].wait_recv()
        for c in q_y[s]:
            c.start()

    lane = lax.broadcasted_iota(jnp.int32, (ROWS, 128), 1)
    marks = jnp.where((lane >= ROPE) & (lane < ROPE + 6), -1.0, 0.0)

    def prepare(t):
        here = slice(ROWS * t, ROWS * (t + 1))
        kt[0:64, here] = jnp.transpose(kvm[here, :].astype(F32))[0:64].astype(BF16)
        kt[64:96, here] = krot[t]
        rot_rows = jnp.concatenate([krot[t].astype(F32), jnp.zeros((ROWS - ROPE, ROWS), F32)], axis=0)
        kvx[here, :] = (jnp.transpose(rot_rows) + marks).astype(BF16)

    prepare(0)
    for i in range(3):
        far[0][i].wait_recv()
        far[2][i].start()
    for c in far[1]:
        c.wait_recv()
    share = [
        copy(LAT_TP + k - 1, latt.at[pl.ds(1, 2), mine], latt.at[pl.ds(1, 2), mine], others(k)) for k in range(1, NTP)
    ]
    for c in share:
        c.start()
    prepare(1)
    prepare(2)

    def tile(s, first, count):
        m = mall[s]
        deltas = []
        for t in range(first, first + count):
            here = slice(ROWS * t, ROWS * (t + 1))
            both = dot(jnp.concatenate([kvm[here, :], kvx[here, :]], axis=1), m)
            ds, mixed = [], []
            for u in range(4):
                probs = jnp.exp2(both[:, 256 * u : 256 * u + 128] * (SCALE * LOG2E))
                ds.append((probs * both[:, 256 * u + 128 : 256 * u + 256]).astype(BF16))
                mixed += [ds[-1], probs.astype(BF16)]
            acc[here, :] += dot_nt(jnp.concatenate(mixed, axis=1), m)
            deltas.append(jnp.concatenate(ds, axis=1))
        deltas = deltas[0] if count == 1 else jnp.concatenate(deltas, axis=0)
        return dot(kt[:, ROWS * first : ROWS * (first + count)], deltas)

    def early(s, carry):
        for u in range(4):
            if u:
                copy(Q_Y + 3 * s + u - 1, qbuf.at[4 * s], qbuf.at[4 * s + u], dev(0, 1)).wait_recv()
            slot, at = 4 * s + u, 256 * u
            mall[s, 0:64, at : at + 128] = qbuf[slot, 0:64, :]
            mall[s, 64:128, at + 128 : at + 256] = qbuf[slot, 64:128, :]
            mall[s, 128:160, at : at + 128] = qbuf[slot, 128:160, :]
            extra = qbuf[slot, 160:176, :].astype(F32)
            mall[s, 160:176, at : at + 128] = jnp.where(row < 3, extra, 0.0).astype(BF16)
            mall[s, 160:176, at + 128 : at + 256] = jnp.where(row >= 3, extra, 0.0).astype(BF16)
        dqp[s] = tile(s, 0, 3)
        return carry

    lax.fori_loop(0, 4, early, 0)

    lane_scale = jnp.where(lane < NOPE, SCALE, 1.0)
    dkv, drot = [], []

    def finish(t):
        here = slice(ROWS * t, ROWS * (t + 1))
        main = acc[here, 0:128] * lane_scale
        hi = main.astype(BF16)
        rots[t] = jnp.transpose(acc[here, 128:256])[0:ROPE] * SCALE
        if t:
            dkvs[t - 1] = hi
            owner = dev(-f_off[t], 0)
            drot.append(copy(DROT + t - 1, rots.at[t], rotr.at[t - 1], owner))
            drot[-1].start()
            dkv.append(copy(DKV + t - 1, dkvs.at[t - 1], dkvr.at[t - 1], owner))
            dkv[-1].start()
        halves[here, 0:128] = hi
        halves[here, 128:256] = (main - hi.astype(F32)).astype(BF16)

    for t in (1, 2, 0):
        finish(t)
    for c in share:
        c.wait_recv()
    wpart = dot(jnp.concatenate([latt[0], latt[1], latt[2]], axis=1), halves[0 : 3 * ROWS, :])
    wpart = wpart[:, 0:128] + wpart[:, 128:256]

    for c in far[2]:
        c.wait_recv()
    share_last = [copy(LAT_TP + 6 + k, latt.at[3, mine], latt.at[3, mine], others(k)) for k in range(1, NTP)]
    for c in share_last:
        c.start()
    prepare(3)

    def late(s, carry):
        total = dqp[s] + tile(s, 3, 1)
        dqp[s] = total
        for u in (1, 2, 3):
            dqb[4 * s + u] = total[:, 128 * u : 128 * u + 128].astype(BF16)
        return carry

    lax.fori_loop(0, 4, late, 0)

    finish(3)
    for c in share_last:
        c.wait_recv()
    more = dot(latt[3], halves[3 * ROWS : 4 * ROWS, :])
    wpart = (wpart + more[:, 0:128] + more[:, 128:256]).reshape(NZ, NY, 8, 128)
    for v in range(NY):
        wsend[v] = wpart[:, v]
    w_y = []
    for u in (1, 2, 3):
        w_y.append(copy(W_Y + u - 1, wsend.at[(y + y_off[u] + NY) % NY], wrecv.at[u - 1], dev(0, y_off[u])))
        w_y[-1].start()

    dq_y = [
        [copy(DQ_Y + 3 * s + u - 1, dqb.at[4 * s + u], dqr.at[3 * s + u - 1], dev(0, -y_off[u])) for u in (1, 2, 3)]
        for s in range(4)
    ]
    for s in (3, 1, 2, 0):
        for c in dq_y[s]:
            c.start()

    def dq_sum(s):
        total = dqp[s, :, 0:128]
        for u in (1, 2, 3):
            dq_y[s][u - 1].wait_recv()
            total = total + dqr[3 * s + u - 1].astype(F32)
        return total

    for c in w_y:
        c.wait_recv()
    wzs[...] = wsend[y] + wrecv[0] + wrecv[1] + wrecv[2]
    w_z = []
    for d in (8, 7, 9, 6, 10, 5, 11, 4, 12, 3, 13, 2, 14, 1, 15):
        w_z.append(copy(W_Z + d - 1, wzs.at[(z + d) % NZ], wzr.at[d - 1], dev(d, 0)))
        w_z[-1].start()

    dq_n = []
    for s in (3, 1, 2):
        dqs[s - 1] = dq_sum(s)
        dq_n.append(copy(DQ_N + s - 1, dqs.at[s - 1], dqz.at[s - 1], dev(-n_off[s], 0)))
        dq_n[-1].start()

    for c in drot:
        c.wait_recv()
    rotx[tp] = rots[0] + rotr[0] + rotr[1] + rotr[2]
    rot = []
    for k in range(1, NTP):
        rot.append(copy(ROT + k - 1, rotx.at[tp], rotx.at[tp], others(k)))
        rot[-1].start()

    for c in dkv:
        c.wait_recv()
    own = acc[0:ROWS, 0:128] * lane_scale
    for t in range(3):
        own = own + dkvr[t].astype(F32)
    own = jnp.transpose(own).astype(BF16)
    dk_ref[...] = own[0:NOPE]
    dv_ref[...] = own[NOPE:128]

    total = dq_sum(0)
    for c in dq_n:
        c.wait_recv()
    dq_ref[...] = ((total + dqz[0] + dqz[1] + dqz[2]) * SCALE).astype(BF16)

    for c in rot:
        c.wait_recv()
    total = rotx[0]
    for k in range(1, NTP):
        total = total + rotx[k]
    drot_ref[...] = total

    for c in w_z:
        c.wait_recv()
    wsum = wzs[z]
    for d in range(1, NZ):
        wsum = wsum + wzr[d - 1]
    dw_ref[...] = wsum

    for c in q_n + share + share_last + dkv + drot + w_y + w_z + rot + dq_n:
        c.wait_send()
    for group in far + q_y + dq_y:
        for c in group:
            c.wait_send()


def hand_over(*refs):
    for src, dst in zip(refs[:5], refs[5:]):
        dst[...] = src[...]


def per_device(queries, latents, rot_key, kv_weight, log_sums, outputs, out_grad):
    vmem = pl.BlockSpec(memory_space=pltpu.VMEM)
    shape = jax.ShapeDtypeStruct
    results = (
        shape((NOPE + ROPE, ROWS), BF16),
        shape((NOPE, ROWS), BF16),
        shape((VAL, ROWS), BF16),
        shape((ROPE, ROWS), F32),
        shape((8, 128), F32),
    )
    made = pl.pallas_call(
        kernel,
        out_shape=results,
        in_specs=[pl.BlockSpec(memory_space=pl.ANY)] * 7,
        out_specs=(vmem,) * 5,
        scratch_shapes=[
            pltpu.VMEM((NOPE + ROPE, ROWS), BF16),
            pltpu.VMEM((ROWS, RANK), BF16),
            pltpu.VMEM((RANK, 128), BF16),
            pltpu.VMEM((1, ROWS), F32),
            pltpu.VMEM((VAL, ROWS), BF16),
            pltpu.VMEM((VAL, ROWS), BF16),
            pltpu.VMEM((16, PACK, ROWS), BF16),
            pltpu.VMEM((4 * ROWS, 128), BF16),
            pltpu.VMEM((4 * ROWS, 128), BF16),
            pltpu.VMEM((4, ROPE, ROWS), BF16),
            pltpu.VMEM((96, 4 * ROWS), BF16),
            pltpu.VMEM((4, RANK, ROWS), BF16),
            pltpu.VMEM((4, 256, 1024), BF16),
            pltpu.VMEM((4 * ROWS, 256), F32),
            pltpu.VMEM((4, 96, 4 * ROWS), F32),
            pltpu.VMEM((16, 96, ROWS), BF16),
            pltpu.VMEM((12, 96, ROWS), BF16),
            pltpu.VMEM((3, 96, ROWS), F32),
            pltpu.VMEM((3, 96, ROWS), F32),
            pltpu.VMEM((3, ROWS, 128), BF16),
            pltpu.VMEM((3, ROWS, 128), BF16),
            pltpu.VMEM((4 * ROWS, 256), BF16),
            pltpu.VMEM((4, ROPE, ROWS), F32),
            pltpu.VMEM((3, ROPE, ROWS), F32),
            pltpu.VMEM((NTP, ROPE, ROWS), F32),
            pltpu.VMEM((NY, NZ, 8, 128), F32),
            pltpu.VMEM((3, NZ, 8, 128), F32),
            pltpu.VMEM((NZ, 8, 128), F32),
            pltpu.VMEM((NZ - 1, 8, 128), F32),
            pltpu.SemaphoreType.DMA((7,)),
            pltpu.SemaphoreType.DMA((COPIES,)),
            pltpu.SemaphoreType.DMA((COPIES,)),
        ],
        compiler_params=pltpu.CompilerParams(collective_id=0, has_side_effects=True),
    )(queries.T, latents, rot_key.T, kv_weight, log_sums.T, outputs.T, out_grad.T)
    dq, dk, dv, drot, dw = pl.pallas_call(
        hand_over, out_shape=results, in_specs=[vmem] * 5, out_specs=(vmem,) * 5
    )(*made)
    return dq.T, dk.T, dv.T, drot.T, dw


def solution(mesh):
    placed = (
        P("sp", "tp"),
        P("sp", None),
        P("sp", None),
        P(None, "tp"),
        P("sp", "tp"),
        P("sp", "tp"),
        P("sp", "tp"),
    )
    return jax.shard_map(
        per_device,
        mesh=mesh,
        in_specs=placed,
        out_specs=(P("sp", "tp"), P("sp", "tp"), P("sp", "tp"), P("sp", None), P("sp", "tp")),
        check_vma=False,
    )
```

```python
import jax
import jax.numpy as jnp
from jax import lax
from jax.experimental import pallas as pl
from jax.experimental.pallas import tpu as pltpu
from jax.sharding import PartitionSpec as P

MESH = pl.DeviceIdType.MESH
F32 = jnp.float32
BF16 = jnp.bfloat16

NOPE = 64
ROPE = 32
VAL = 64
RANK = 512
ROWS = 128
NY = 4
NZ = 16
NTP = 8
PART = RANK // NTP
PACK = 176
SCALE = (NOPE + ROPE) ** -0.5
LOG2E = 1.4426950408889634

K_FAR = 0
K_ROT = 3
LAT = 6
LAT_TP = 9
Q_N = 23
Q_Y = 26
DQ_Y = 38
DQ_N = 50
DKV = 53
DROT = 56
W_Y = 59
W_Z = 62
ROT = 77
COPIES = 84


def three(x):
    hi = x.astype(BF16)
    rest = x - hi.astype(F32)
    mid = rest.astype(BF16)
    low = (rest - mid.astype(F32)).astype(BF16)
    return [hi.astype(F32), mid.astype(F32), low.astype(F32)]


def dot(a, b):
    return jnp.dot(a, b, preferred_element_type=F32)


def dot_nt(a, b):
    return lax.dot_general(a, b, (((1,), (1,)), ((), ())), preferred_element_type=F32)


def kernel(
    q_hbm, lat_hbm, rot_hbm, w_hbm, lse_hbm, o_hbm, do_hbm,
    dq_ref, dk_ref, dv_ref, drot_ref, dw_ref,
    q_ref, lat_ref, w_ref, lse_ref, o_ref, do_ref,
    qbuf, kvm, kvx, krot, kt, latt, mall, acc, dqp, dqb, dqr, dqs, dqz, dkvs, dkvr, halves, rot_own, rots, rotr, rotx,
    wsend, wnarrow, wrecv, wzs, wzr,
    isem, ssem, rsem,
):
    sp = lax.axis_index("sp")
    tp = lax.axis_index("tp")
    z = sp // NY
    y = sp % NY
    sign = 1 - 2 * (z % 2)

    def dev(dz, dy):
        return (((z + dz + NZ) % NZ) * NY + (y + dy + NY) % NY, tp)

    y_off = (0, 1, -1, 2)
    n_off = (0, 1, -1, 2 * sign)
    f_off = (0, 4 * sign, -4 * sign, 8)

    def copy(number, src, dst, device):
        return pltpu.make_async_remote_copy(
            src_ref=src, dst_ref=dst, send_sem=ssem.at[number], recv_sem=rsem.at[number],
            device_id=device, device_id_type=MESH,
        )

    def others(k):
        return (sp, (tp + k) % NTP)

    def rows_of(t):
        return pl.ds(ROWS * t, ROWS)

    loads = [
        pltpu.make_async_copy(src, dst, isem.at[i])
        for i, (src, dst) in enumerate((
            (lat_hbm, lat_ref), (w_hbm, w_ref), (rot_hbm, krot.at[0]),
            (o_hbm, o_ref), (do_hbm, do_ref), (q_hbm, q_ref), (lse_hbm, lse_ref),
        ))
    ]
    barrier = pltpu.get_barrier_semaphore()
    greet = [dev(d, 0) for d in (4, -4, 1, -1, 2, -2)] + [dev(0, d) for d in (1, -1, 2)]
    greet += [others(k) for k in range(1, NTP)]
    for device in greet:
        pl.semaphore_signal(barrier, inc=1, device_id=device, device_id_type=MESH)
    for c in loads:
        c.start()
    mall[...] = jnp.zeros_like(mall)
    acc[...] = jnp.zeros_like(acc)

    for c in loads[0:3]:
        c.wait()
    kvm[0:ROWS, :] = dot(lat_ref[...], w_ref[...]).astype(BF16)
    latt[0] = jnp.transpose(lat_ref[...].astype(F32)).astype(BF16)

    for c in loads[3:7]:
        c.wait()
    delta = jnp.sum(o_ref[...].astype(F32) * do_ref[...].astype(F32), axis=0, keepdims=True)
    lse = lse_ref[...] * (1.0 / SCALE)
    row = lax.broadcasted_iota(jnp.int32, (16, ROWS), 0)
    aux = jnp.zeros((16, ROWS), F32)
    for i, piece in enumerate(three(lse) + three(delta)):
        aux = jnp.where(row == i, jnp.broadcast_to(piece, (16, ROWS)), aux)
    qbuf[0, 0:64, :] = q_ref[0:64, :]
    qbuf[0, 64:128, :] = do_ref[...]
    qbuf[0, 128:160, :] = q_ref[64:96, :]
    qbuf[0, 160:176, :] = aux.astype(BF16)

    pl.semaphore_wait(barrier, len(greet))

    mine = pl.ds(PART * tp, PART)
    far = [
        [
            copy(LAT + t - 1, latt.at[a, mine], latt.at[t, mine], device),
            copy(K_ROT + t - 1, krot.at[a], krot.at[t], device),
            copy(K_FAR + t - 1, kvm.at[rows_of(a)], kvm.at[rows_of(t)], device),
        ]
        for t, a, device in ((1, 0, dev(4 * sign, 0)), (2, 0, dev(-4 * sign, 0)), (3, 1, dev(4 * sign, 0)))
    ]
    q_n = [copy(Q_N + s - 1, qbuf.at[0], qbuf.at[4 * s], dev(n_off[s], 0)) for s in (1, 2, 3)]
    q_y = [
        [copy(Q_Y + 3 * s + u - 1, qbuf.at[4 * s], qbuf.at[4 * s + u], dev(0, y_off[u])) for u in (1, 2, 3)]
        for s in range(4)
    ]
    for c in q_n + q_y[0] + far[0] + far[1]:
        c.start()
    for s in (1, 2, 3):
        q_n[s - 1].wait_recv()
        for c in q_y[s]:
            c.start()

    lane = lax.broadcasted_iota(jnp.int32, (ROWS, 128), 1)
    marks = jnp.where((lane >= ROPE) & (lane < ROPE + 6), -1.0, 0.0)

    def prepare(t):
        here = slice(ROWS * t, ROWS * (t + 1))
        kt[0:64, here] = jnp.transpose(kvm[here, :].astype(F32))[0:64].astype(BF16)
        kt[64:96, here] = krot[t]
        rot_rows = jnp.concatenate([krot[t].astype(F32), jnp.zeros((ROWS - ROPE, ROWS), F32)], axis=0)
        kvx[here, :] = (jnp.transpose(rot_rows) + marks).astype(BF16)

    prepare(0)
    for i in range(3):
        far[0][i].wait_recv()
        far[2][i].start()
    for c in far[1]:
        c.wait_recv()
    share = [
        copy(LAT_TP + k - 1, latt.at[pl.ds(1, 2), mine], latt.at[pl.ds(1, 2), mine], others(k)) for k in range(1, NTP)
    ]
    for c in share:
        c.start()
    prepare(1)
    prepare(2)
    far[2][0].wait_recv()
    share_last = [copy(LAT_TP + 6 + k, latt.at[3, mine], latt.at[3, mine], others(k)) for k in range(1, NTP)]
    for c in share_last:
        c.start()

    def tile(s, first, count):
        m = mall[s]
        deltas = []
        for t in range(first, first + count):
            here = slice(ROWS * t, ROWS * (t + 1))
            both = dot(jnp.concatenate([kvm[here, :], kvx[here, :]], axis=1), m)
            ds, mixed = [], []
            for u in range(4):
                probs = jnp.exp2(both[:, 256 * u : 256 * u + 128] * (SCALE * LOG2E))
                ds.append((probs * both[:, 256 * u + 128 : 256 * u + 256]).astype(BF16))
                mixed += [ds[-1], probs.astype(BF16)]
            acc[here, :] += dot_nt(jnp.concatenate(mixed, axis=1), m)
            deltas.append(jnp.concatenate(ds, axis=1))
        deltas = deltas[0] if count == 1 else jnp.concatenate(deltas, axis=0)
        return dot(kt[:, ROWS * first : ROWS * (first + count)], deltas)

    def early(s, carry):
        for u in range(4):
            if u:
                copy(Q_Y + 3 * s + u - 1, qbuf.at[4 * s], qbuf.at[4 * s + u], dev(0, 1)).wait_recv()
            slot, at = 4 * s + u, 256 * u
            mall[s, 0:64, at : at + 128] = qbuf[slot, 0:64, :]
            mall[s, 64:128, at + 128 : at + 256] = qbuf[slot, 64:128, :]
            mall[s, 128:160, at : at + 128] = qbuf[slot, 128:160, :]
            extra = qbuf[slot, 160:176, :].astype(F32)
            mall[s, 160:176, at : at + 128] = jnp.where(row < 3, extra, 0.0).astype(BF16)
            mall[s, 160:176, at + 128 : at + 256] = jnp.where(row >= 3, extra, 0.0).astype(BF16)
        dqp[s] = tile(s, 0, 3)
        return carry

    lax.fori_loop(0, 4, early, 0)

    lane_scale = jnp.where(lane < NOPE, SCALE, 1.0)
    dkv, drot = [], []

    def finish(t):
        here = slice(ROWS * t, ROWS * (t + 1))
        main = acc[here, 0:128] * lane_scale
        hi = main.astype(BF16)
        rot_part = jnp.transpose(acc[here, 128:256])[0:ROPE] * SCALE
        if t == 0:
            rot_own[...] = rot_part
        else:
            rots[t - 1] = rot_part.astype(BF16)
            dkvs[t - 1] = hi
            owner = dev(-f_off[t], 0)
            drot.append(copy(DROT + t - 1, rots.at[t - 1], rotr.at[t - 1], owner))
            drot[-1].start()
            dkv.append(copy(DKV + t - 1, dkvs.at[t - 1], dkvr.at[t - 1], owner))
            dkv[-1].start()
        halves[here, 0:128] = hi
        halves[here, 128:256] = (main - hi.astype(F32)).astype(BF16)

    for t in (1, 2, 0):
        finish(t)
    for c in share:
        c.wait_recv()
    wpart = dot(jnp.concatenate([latt[0], latt[1], latt[2]], axis=1), halves[0 : 3 * ROWS, :])
    wpart = wpart[:, 0:128] + wpart[:, 128:256]

    for c in far[2][1:]:
        c.wait_recv()
    prepare(3)

    def late(s, carry):
        total = dqp[s] + tile(s, 3, 1)
        dqp[s] = total
        for u in (1, 2, 3):
            dqb[4 * s + u] = total[:, 128 * u : 128 * u + 128].astype(BF16)
        return carry

    lax.fori_loop(0, 4, late, 0)

    finish(3)
    for c in share_last:
        c.wait_recv()
    more = dot(latt[3], halves[3 * ROWS : 4 * ROWS, :])
    wpart = (wpart + more[:, 0:128] + more[:, 128:256]).reshape(NZ, NY, 8, 128)
    for v in range(NY):
        wsend[v] = wpart[:, v].reshape(NZ * 8, 128)
    wnarrow[...] = wsend[...].astype(BF16)
    w_y = []
    for u in (1, 2, 3):
        w_y.append(copy(W_Y + u - 1, wnarrow.at[(y + y_off[u] + NY) % NY], wrecv.at[u - 1], dev(0, y_off[u])))
        w_y[-1].start()

    dq_y = [
        [copy(DQ_Y + 3 * s + u - 1, dqb.at[4 * s + u], dqr.at[3 * s + u - 1], dev(0, -y_off[u])) for u in (1, 2, 3)]
        for s in range(4)
    ]
    for s in (3, 1, 2, 0):
        for c in dq_y[s]:
            c.start()

    def dq_sum(s):
        total = dqp[s, :, 0:128]
        for u in (1, 2, 3):
            dq_y[s][u - 1].wait_recv()
            total = total + dqr[3 * s + u - 1].astype(F32)
        return total

    for c in w_y:
        c.wait_recv()
    wsum = wsend[y]
    for u in range(3):
        wsum = wsum + wrecv[u].astype(F32)
    wzs[...] = wsum.reshape(NZ, 8, 128)
    w_z = []
    for d in (8, 7, 9, 6, 10, 5, 11, 4, 12, 3, 13, 2, 14, 1, 15):
        w_z.append(copy(W_Z + d - 1, wzs.at[(z + d) % NZ], wzr.at[d - 1], dev(d, 0)))
        w_z[-1].start()

    for c in drot:
        c.wait_recv()
    total = rot_own[...]
    for t in range(3):
        total = total + rotr[t].astype(F32)
    rotx[tp] = total.astype(BF16)
    rot = []
    for k in range(1, NTP):
        rot.append(copy(ROT + k - 1, rotx.at[tp], rotx.at[tp], others(k)))
        rot[-1].start()

    dq_n = []
    for s in (3, 1, 2):
        dqs[s - 1] = dq_sum(s)
        dq_n.append(copy(DQ_N + s - 1, dqs.at[s - 1], dqz.at[s - 1], dev(-n_off[s], 0)))
        dq_n[-1].start()

    for c in dkv:
        c.wait_recv()
    own = acc[0:ROWS, 0:128] * lane_scale
    for t in range(3):
        own = own + dkvr[t].astype(F32)
    own = jnp.transpose(own).astype(BF16)
    dk_ref[...] = own[0:NOPE]
    dv_ref[...] = own[NOPE:128]

    total = dq_sum(0)
    for c in dq_n:
        c.wait_recv()
    dq_ref[...] = ((total + dqz[0] + dqz[1] + dqz[2]) * SCALE).astype(BF16)

    for c in rot:
        c.wait_recv()
    total = rotx[0].astype(F32)
    for k in range(1, NTP):
        total = total + rotx[k].astype(F32)
    drot_ref[...] = total

    for c in w_z:
        c.wait_recv()
    wsum = wzs[z]
    for d in range(1, NZ):
        wsum = wsum + wzr[d - 1]
    dw_ref[...] = wsum

    for c in q_n + share + share_last + dkv + drot + w_y + w_z + rot + dq_n:
        c.wait_send()
    for group in far + q_y + dq_y:
        for c in group:
            c.wait_send()


def hand_over(*refs):
    for src, dst in zip(refs[:5], refs[5:]):
        dst[...] = src[...]


def per_device(queries, latents, rot_key, kv_weight, log_sums, outputs, out_grad):
    vmem = pl.BlockSpec(memory_space=pltpu.VMEM)
    shape = jax.ShapeDtypeStruct
    results = (
        shape((NOPE + ROPE, ROWS), BF16),
        shape((NOPE, ROWS), BF16),
        shape((VAL, ROWS), BF16),
        shape((ROPE, ROWS), F32),
        shape((8, 128), F32),
    )
    made = pl.pallas_call(
        kernel,
        out_shape=results,
        in_specs=[pl.BlockSpec(memory_space=pl.ANY)] * 7,
        out_specs=(vmem,) * 5,
        scratch_shapes=[
            pltpu.VMEM((NOPE + ROPE, ROWS), BF16),
            pltpu.VMEM((ROWS, RANK), BF16),
            pltpu.VMEM((RANK, 128), BF16),
            pltpu.VMEM((1, ROWS), F32),
            pltpu.VMEM((VAL, ROWS), BF16),
            pltpu.VMEM((VAL, ROWS), BF16),
            pltpu.VMEM((16, PACK, ROWS), BF16),
            pltpu.VMEM((4 * ROWS, 128), BF16),
            pltpu.VMEM((4 * ROWS, 128), BF16),
            pltpu.VMEM((4, ROPE, ROWS), BF16),
            pltpu.VMEM((96, 4 * ROWS), BF16),
            pltpu.VMEM((4, RANK, ROWS), BF16),
            pltpu.VMEM((4, 256, 1024), BF16),
            pltpu.VMEM((4 * ROWS, 256), F32),
            pltpu.VMEM((4, 96, 4 * ROWS), F32),
            pltpu.VMEM((16, 96, ROWS), BF16),
            pltpu.VMEM((12, 96, ROWS), BF16),
            pltpu.VMEM((3, 96, ROWS), F32),
            pltpu.VMEM((3, 96, ROWS), F32),
            pltpu.VMEM((3, ROWS, 128), BF16),
            pltpu.VMEM((3, ROWS, 128), BF16),
            pltpu.VMEM((4 * ROWS, 256), BF16),
            pltpu.VMEM((ROPE, ROWS), F32),
            pltpu.VMEM((3, ROPE, ROWS), BF16),
            pltpu.VMEM((3, ROPE, ROWS), BF16),
            pltpu.VMEM((NTP, ROPE, ROWS), BF16),
            pltpu.VMEM((NY, NZ * 8, 128), F32),
            pltpu.VMEM((NY, NZ * 8, 128), BF16),
            pltpu.VMEM((3, NZ * 8, 128), BF16),
            pltpu.VMEM((NZ, 8, 128), F32),
            pltpu.VMEM((NZ - 1, 8, 128), F32),
            pltpu.SemaphoreType.DMA((7,)),
            pltpu.SemaphoreType.DMA((COPIES,)),
            pltpu.SemaphoreType.DMA((COPIES,)),
        ],
        compiler_params=pltpu.CompilerParams(collective_id=0, has_side_effects=True),
    )(queries.T, latents, rot_key.T, kv_weight, log_sums.T, outputs.T, out_grad.T)
    dq, dk, dv, drot, dw = pl.pallas_call(
        hand_over, out_shape=results, in_specs=[vmem] * 5, out_specs=(vmem,) * 5
    )(*made)
    return dq.T, dk.T, dv.T, drot.T, dw


def solution(mesh):
    placed = (
        P("sp", "tp"),
        P("sp", None),
        P("sp", None),
        P(None, "tp"),
        P("sp", "tp"),
        P("sp", "tp"),
        P("sp", "tp"),
    )
    return jax.shard_map(
        per_device,
        mesh=mesh,
        in_specs=placed,
        out_specs=(P("sp", "tp"), P("sp", "tp"), P("sp", "tp"), P("sp", None), P("sp", "tp")),
        check_vma=False,
    )
```

```python
import jax
import jax.numpy as jnp
from jax import lax
from jax.experimental import pallas as pl
from jax.experimental.pallas import tpu as pltpu
from jax.sharding import PartitionSpec as P

MESH = pl.DeviceIdType.MESH
F32 = jnp.float32
BF16 = jnp.bfloat16

NOPE = 64
ROPE = 32
VAL = 64
RANK = 512
ROWS = 128
NY = 4
NZ = 16
NTP = 8
PART = RANK // NTP
PACK = 176
SCALE = (NOPE + ROPE) ** -0.5
LOG2E = 1.4426950408889634

K_FAR = 0
K_ROT = 3
LAT = 6
LAT_TP = 9
Q_N = 23
Q_Y = 26
DQ_Y = 38
DQ_N = 50
DKV = 53
DROT = 56
W_Y = 59
W_Z = 62
ROT = 77
COPIES = 84


def three(x):
    hi = x.astype(BF16)
    rest = x - hi.astype(F32)
    mid = rest.astype(BF16)
    low = (rest - mid.astype(F32)).astype(BF16)
    return [hi.astype(F32), mid.astype(F32), low.astype(F32)]


def dot(a, b):
    return jnp.dot(a, b, preferred_element_type=F32)


def dot_nt(a, b):
    return lax.dot_general(a, b, (((1,), (1,)), ((), ())), preferred_element_type=F32)


def kernel(
    q_hbm, lat_hbm, rot_hbm, w_hbm, lse_hbm, o_hbm, do_hbm,
    dq_ref, dk_ref, dv_ref, drot_ref, dw_ref,
    q_ref, lat_ref, w_ref, lse_ref, o_ref, do_ref,
    qbuf, kvm, kvx, krot, kt, latt, mall, acc, dqp, dqb, dqr, dqs, dqz, dkvs, dkvr, halves, rot_own, rots, rotr, rotx,
    wsend, wnarrow, wrecv, wzs, wzb, wzr,
    isem, ssem, rsem,
):
    sp = lax.axis_index("sp")
    tp = lax.axis_index("tp")
    z = sp // NY
    y = sp % NY
    sign = 1 - 2 * (z % 2)

    def dev(dz, dy):
        return (((z + dz + NZ) % NZ) * NY + (y + dy + NY) % NY, tp)

    y_off = (0, 1, -1, 2)
    n_off = (0, 1, -1, 2 * sign)
    f_off = (0, 4 * sign, -4 * sign, 8)

    def copy(number, src, dst, device):
        return pltpu.make_async_remote_copy(
            src_ref=src, dst_ref=dst, send_sem=ssem.at[number], recv_sem=rsem.at[number],
            device_id=device, device_id_type=MESH,
        )

    def others(k):
        return (sp, (tp + k) % NTP)

    def rows_of(t):
        return pl.ds(ROWS * t, ROWS)

    loads = [
        pltpu.make_async_copy(src, dst, isem.at[i])
        for i, (src, dst) in enumerate((
            (lat_hbm, lat_ref), (w_hbm, w_ref), (rot_hbm, krot.at[0]),
            (o_hbm, o_ref), (do_hbm, do_ref), (q_hbm, q_ref), (lse_hbm, lse_ref),
        ))
    ]
    barrier = pltpu.get_barrier_semaphore()
    greet = [dev(d, 0) for d in (4, -4, 1, -1, 2, -2)] + [dev(0, d) for d in (1, -1, 2)]
    greet += [others(k) for k in range(1, NTP)]
    for device in greet:
        pl.semaphore_signal(barrier, inc=1, device_id=device, device_id_type=MESH)
    for c in loads:
        c.start()
    mall[...] = jnp.zeros_like(mall)
    acc[...] = jnp.zeros_like(acc)

    for c in loads[0:3]:
        c.wait()
    kvm[0:ROWS, :] = dot(lat_ref[...], w_ref[...]).astype(BF16)
    latt[0] = jnp.transpose(lat_ref[...].astype(F32)).astype(BF16)

    for c in loads[3:7]:
        c.wait()
    delta = jnp.sum(o_ref[...].astype(F32) * do_ref[...].astype(F32), axis=0, keepdims=True)
    lse = lse_ref[...] * (1.0 / SCALE)
    row = lax.broadcasted_iota(jnp.int32, (16, ROWS), 0)
    aux = jnp.zeros((16, ROWS), F32)
    for i, piece in enumerate(three(lse) + three(delta)):
        aux = jnp.where(row == i, jnp.broadcast_to(piece, (16, ROWS)), aux)
    qbuf[0, 0:64, :] = q_ref[0:64, :]
    qbuf[0, 64:128, :] = do_ref[...]
    qbuf[0, 128:160, :] = q_ref[64:96, :]
    qbuf[0, 160:176, :] = aux.astype(BF16)

    pl.semaphore_wait(barrier, len(greet))

    mine = pl.ds(PART * tp, PART)
    far = [
        [
            copy(LAT + t - 1, latt.at[a, mine], latt.at[t, mine], device),
            copy(K_ROT + t - 1, krot.at[a], krot.at[t], device),
            copy(K_FAR + t - 1, kvm.at[rows_of(a)], kvm.at[rows_of(t)], device),
        ]
        for t, a, device in ((1, 0, dev(4 * sign, 0)), (2, 0, dev(-4 * sign, 0)), (3, 1, dev(4 * sign, 0)))
    ]
    q_n = [copy(Q_N + s - 1, qbuf.at[0], qbuf.at[4 * s], dev(n_off[s], 0)) for s in (1, 2, 3)]
    q_y = [
        [copy(Q_Y + 3 * s + u - 1, qbuf.at[4 * s], qbuf.at[4 * s + u], dev(0, y_off[u])) for u in (1, 2, 3)]
        for s in range(4)
    ]
    for c in q_n + q_y[0] + far[0] + far[1]:
        c.start()
    for s in (1, 2, 3):
        q_n[s - 1].wait_recv()
        for c in q_y[s]:
            c.start()

    lane = lax.broadcasted_iota(jnp.int32, (ROWS, 128), 1)
    marks = jnp.where((lane >= ROPE) & (lane < ROPE + 6), -1.0, 0.0)

    def prepare(t):
        here = slice(ROWS * t, ROWS * (t + 1))
        kt[0:64, here] = jnp.transpose(kvm[here, :].astype(F32))[0:64].astype(BF16)
        kt[64:96, here] = krot[t]
        rot_rows = jnp.concatenate([krot[t].astype(F32), jnp.zeros((ROWS - ROPE, ROWS), F32)], axis=0)
        kvx[here, :] = (jnp.transpose(rot_rows) + marks).astype(BF16)

    prepare(0)
    for i in range(3):
        far[0][i].wait_recv()
        far[2][i].start()
    for c in far[1]:
        c.wait_recv()
    share = [
        copy(LAT_TP + k - 1, latt.at[pl.ds(1, 2), mine], latt.at[pl.ds(1, 2), mine], others(k)) for k in range(1, NTP)
    ]
    for c in share:
        c.start()
    prepare(1)
    prepare(2)
    far[2][0].wait_recv()
    share_last = [copy(LAT_TP + 6 + k, latt.at[3, mine], latt.at[3, mine], others(k)) for k in range(1, NTP)]
    for c in share_last:
        c.start()

    def tile(s, first, count):
        m = mall[s]
        deltas = []
        for t in range(first, first + count):
            here = slice(ROWS * t, ROWS * (t + 1))
            both = dot(jnp.concatenate([kvm[here, :], kvx[here, :]], axis=1), m)
            ds, mixed = [], []
            for u in range(4):
                probs = jnp.exp2(both[:, 256 * u : 256 * u + 128] * (SCALE * LOG2E))
                ds.append((probs * both[:, 256 * u + 128 : 256 * u + 256]).astype(BF16))
                mixed += [ds[-1], probs.astype(BF16)]
            acc[here, :] += dot_nt(jnp.concatenate(mixed, axis=1), m)
            deltas.append(jnp.concatenate(ds, axis=1))
        deltas = deltas[0] if count == 1 else jnp.concatenate(deltas, axis=0)
        return dot(kt[:, ROWS * first : ROWS * (first + count)], deltas)

    def early(s, carry):
        for u in range(4):
            if u:
                copy(Q_Y + 3 * s + u - 1, qbuf.at[4 * s], qbuf.at[4 * s + u], dev(0, 1)).wait_recv()
            slot, at = 4 * s + u, 256 * u
            mall[s, 0:64, at : at + 128] = qbuf[slot, 0:64, :]
            mall[s, 64:128, at + 128 : at + 256] = qbuf[slot, 64:128, :]
            mall[s, 128:160, at : at + 128] = qbuf[slot, 128:160, :]
            extra = qbuf[slot, 160:176, :].astype(F32)
            mall[s, 160:176, at : at + 128] = jnp.where(row < 3, extra, 0.0).astype(BF16)
            mall[s, 160:176, at + 128 : at + 256] = jnp.where(row >= 3, extra, 0.0).astype(BF16)
        dqp[s] = tile(s, 0, 3)
        return carry

    lax.fori_loop(0, 4, early, 0)

    lane_scale = jnp.where(lane < NOPE, SCALE, 1.0)
    dkv, drot = [], []

    def finish(t):
        here = slice(ROWS * t, ROWS * (t + 1))
        main = acc[here, 0:128] * lane_scale
        hi = main.astype(BF16)
        rot_part = jnp.transpose(acc[here, 128:256])[0:ROPE] * SCALE
        if t == 0:
            rot_own[...] = rot_part
        else:
            rots[t - 1] = rot_part.astype(BF16)
            dkvs[t - 1] = hi
            owner = dev(-f_off[t], 0)
            drot.append(copy(DROT + t - 1, rots.at[t - 1], rotr.at[t - 1], owner))
            drot[-1].start()
            dkv.append(copy(DKV + t - 1, dkvs.at[t - 1], dkvr.at[t - 1], owner))
            dkv[-1].start()
        halves[here, 0:128] = hi
        halves[here, 128:256] = (main - hi.astype(F32)).astype(BF16)

    for t in (1, 2):
        finish(t)

    for c in far[2][1:]:
        c.wait_recv()
    prepare(3)

    def late(s, carry):
        total = dqp[s] + tile(s, 3, 1)
        dqp[s] = total
        for u in (1, 2, 3):
            dqb[4 * s + u] = total[:, 128 * u : 128 * u + 128].astype(BF16)
        return carry

    lax.fori_loop(0, 4, late, 0)

    finish(3)
    finish(0)
    for c in share + share_last:
        c.wait_recv()
    wpart = dot(jnp.concatenate([latt[0], latt[1], latt[2], latt[3]], axis=1), halves[...])
    wpart = (wpart[:, 0:128] + wpart[:, 128:256]).reshape(NZ, NY, 8, 128)
    for v in range(NY):
        wsend[v] = wpart[:, v].reshape(NZ * 8, 128)
    wnarrow[...] = wsend[...].astype(BF16)
    w_y = []
    for u in (1, 2, 3):
        w_y.append(copy(W_Y + u - 1, wnarrow.at[(y + y_off[u] + NY) % NY], wrecv.at[u - 1], dev(0, y_off[u])))
        w_y[-1].start()

    dq_y = [
        [copy(DQ_Y + 3 * s + u - 1, dqb.at[4 * s + u], dqr.at[3 * s + u - 1], dev(0, -y_off[u])) for u in (1, 2, 3)]
        for s in range(4)
    ]
    for s in (3, 1, 2, 0):
        for c in dq_y[s]:
            c.start()

    def dq_sum(s):
        total = dqp[s, :, 0:128]
        for u in (1, 2, 3):
            dq_y[s][u - 1].wait_recv()
            total = total + dqr[3 * s + u - 1].astype(F32)
        return total

    for c in w_y:
        c.wait_recv()
    wsum = wsend[y]
    for u in range(3):
        wsum = wsum + wrecv[u].astype(F32)
    wzs[...] = wsum.reshape(NZ, 8, 128)
    wzb[...] = wzs[...].astype(BF16)
    w_z = []
    for d in (8, 7, 9, 6, 10, 5, 11, 4, 12, 3, 13, 2, 14, 1, 15):
        w_z.append(copy(W_Z + d - 1, wzb.at[(z + d) % NZ], wzr.at[d - 1], dev(d, 0)))
        w_z[-1].start()

    for c in drot:
        c.wait_recv()
    total = rot_own[...]
    for t in range(3):
        total = total + rotr[t].astype(F32)
    rotx[tp] = total.astype(BF16)
    rot = []
    for k in range(1, NTP):
        rot.append(copy(ROT + k - 1, rotx.at[tp], rotx.at[tp], others(k)))
        rot[-1].start()

    dq_n = []
    for s in (3, 1, 2):
        dqs[s - 1] = dq_sum(s)
        dq_n.append(copy(DQ_N + s - 1, dqs.at[s - 1], dqz.at[s - 1], dev(-n_off[s], 0)))
        dq_n[-1].start()

    for c in dkv:
        c.wait_recv()
    own = acc[0:ROWS, 0:128] * lane_scale
    for t in range(3):
        own = own + dkvr[t].astype(F32)
    own = jnp.transpose(own).astype(BF16)
    dk_ref[...] = own[0:NOPE]
    dv_ref[...] = own[NOPE:128]

    total = dq_sum(0)
    for c in dq_n:
        c.wait_recv()
    dq_ref[...] = ((total + dqz[0] + dqz[1] + dqz[2]) * SCALE).astype(BF16)

    for c in rot:
        c.wait_recv()
    total = rotx[0].astype(F32)
    for k in range(1, NTP):
        total = total + rotx[k].astype(F32)
    drot_ref[...] = total

    for c in w_z:
        c.wait_recv()
    wsum = wzs[z]
    for d in range(1, NZ):
        wsum = wsum + wzr[d - 1].astype(F32)
    dw_ref[...] = wsum

    for c in q_n + share + share_last + dkv + drot + w_y + w_z + rot + dq_n:
        c.wait_send()
    for group in far + q_y + dq_y:
        for c in group:
            c.wait_send()


def hand_over(*refs):
    for src, dst in zip(refs[:5], refs[5:]):
        dst[...] = src[...]


def per_device(queries, latents, rot_key, kv_weight, log_sums, outputs, out_grad):
    vmem = pl.BlockSpec(memory_space=pltpu.VMEM)
    shape = jax.ShapeDtypeStruct
    results = (
        shape((NOPE + ROPE, ROWS), BF16),
        shape((NOPE, ROWS), BF16),
        shape((VAL, ROWS), BF16),
        shape((ROPE, ROWS), F32),
        shape((8, 128), F32),
    )
    made = pl.pallas_call(
        kernel,
        out_shape=results,
        in_specs=[pl.BlockSpec(memory_space=pl.ANY)] * 7,
        out_specs=(vmem,) * 5,
        scratch_shapes=[
            pltpu.VMEM((NOPE + ROPE, ROWS), BF16),
            pltpu.VMEM((ROWS, RANK), BF16),
            pltpu.VMEM((RANK, 128), BF16),
            pltpu.VMEM((1, ROWS), F32),
            pltpu.VMEM((VAL, ROWS), BF16),
            pltpu.VMEM((VAL, ROWS), BF16),
            pltpu.VMEM((16, PACK, ROWS), BF16),
            pltpu.VMEM((4 * ROWS, 128), BF16),
            pltpu.VMEM((4 * ROWS, 128), BF16),
            pltpu.VMEM((4, ROPE, ROWS), BF16),
            pltpu.VMEM((96, 4 * ROWS), BF16),
            pltpu.VMEM((4, RANK, ROWS), BF16),
            pltpu.VMEM((4, 256, 1024), BF16),
            pltpu.VMEM((4 * ROWS, 256), F32),
            pltpu.VMEM((4, 96, 4 * ROWS), F32),
            pltpu.VMEM((16, 96, ROWS), BF16),
            pltpu.VMEM((12, 96, ROWS), BF16),
            pltpu.VMEM((3, 96, ROWS), F32),
            pltpu.VMEM((3, 96, ROWS), F32),
            pltpu.VMEM((3, ROWS, 128), BF16),
            pltpu.VMEM((3, ROWS, 128), BF16),
            pltpu.VMEM((4 * ROWS, 256), BF16),
            pltpu.VMEM((ROPE, ROWS), F32),
            pltpu.VMEM((3, ROPE, ROWS), BF16),
            pltpu.VMEM((3, ROPE, ROWS), BF16),
            pltpu.VMEM((NTP, ROPE, ROWS), BF16),
            pltpu.VMEM((NY, NZ * 8, 128), F32),
            pltpu.VMEM((NY, NZ * 8, 128), BF16),
            pltpu.VMEM((3, NZ * 8, 128), BF16),
            pltpu.VMEM((NZ, 8, 128), F32),
            pltpu.VMEM((NZ, 8, 128), BF16),
            pltpu.VMEM((NZ - 1, 8, 128), BF16),
            pltpu.SemaphoreType.DMA((7,)),
            pltpu.SemaphoreType.DMA((COPIES,)),
            pltpu.SemaphoreType.DMA((COPIES,)),
        ],
        compiler_params=pltpu.CompilerParams(collective_id=0, has_side_effects=True),
    )(queries.T, latents, rot_key.T, kv_weight, log_sums.T, outputs.T, out_grad.T)
    dq, dk, dv, drot, dw = pl.pallas_call(
        hand_over, out_shape=results, in_specs=[vmem] * 5, out_specs=(vmem,) * 5
    )(*made)
    return dq.T, dk.T, dv.T, drot.T, dw


def solution(mesh):
    placed = (
        P("sp", "tp"),
        P("sp", None),
        P("sp", None),
        P(None, "tp"),
        P("sp", "tp"),
        P("sp", "tp"),
        P("sp", "tp"),
    )
    return jax.shard_map(
        per_device,
        mesh=mesh,
        in_specs=placed,
        out_specs=(P("sp", "tp"), P("sp", "tp"), P("sp", "tp"), P("sp", None), P("sp", "tp")),
        check_vma=False,
    )
```

```python
import jax
import jax.numpy as jnp
from jax import lax
from jax.experimental import pallas as pl
from jax.experimental.pallas import tpu as pltpu
from jax.sharding import PartitionSpec as P

MESH = pl.DeviceIdType.MESH
F32 = jnp.float32
BF16 = jnp.bfloat16

NOPE = 64
ROPE = 32
VAL = 64
RANK = 512
ROWS = 128
NY = 4
NZ = 16
NTP = 8
PART = RANK // NTP
PACK = 176
SCALE = (NOPE + ROPE) ** -0.5
LOG2E = 1.4426950408889634

K_FAR = 0
K_ROT = 3
LAT = 6
LAT_TP = 9
Q_N = 23
Q_Y = 26
DQ_Y = 38
DQ_N = 50
DKV = 53
DROT = 56
W_Y = 59
W_Z = 62
ROT = 77
COPIES = 84


def three(x):
    hi = x.astype(BF16)
    rest = x - hi.astype(F32)
    mid = rest.astype(BF16)
    low = (rest - mid.astype(F32)).astype(BF16)
    return [hi.astype(F32), mid.astype(F32), low.astype(F32)]


def dot(a, b):
    return jnp.dot(a, b, preferred_element_type=F32)


def dot_nt(a, b):
    return lax.dot_general(a, b, (((1,), (1,)), ((), ())), preferred_element_type=F32)


def kernel(
    q_hbm, lat_hbm, rot_hbm, w_hbm, lse_hbm, o_hbm, do_hbm,
    dq_ref, dk_ref, dv_ref, drot_ref, dw_ref,
    q_ref, lat_ref, w_ref, lse_ref, o_ref, do_ref,
    qbuf, kvm, kvx, krot, kt, latt, mall, acc, dqp, dqb, dqr, dqs, dqz, dkvs, dkvr, halves, rot_own, rots, rotr, rotx,
    wsend, wnarrow, wrecv, wzs, wzb, wzr,
    isem, ssem, rsem,
):
    sp = lax.axis_index("sp")
    tp = lax.axis_index("tp")
    z = sp // NY
    y = sp % NY
    sign = 1 - 2 * (z % 2)

    def dev(dz, dy):
        return (((z + dz + NZ) % NZ) * NY + (y + dy + NY) % NY, tp)

    y_off = (0, 1, -1, 2)
    n_off = (0, 1, -1, 2 * sign)
    f_off = (0, 4 * sign, -4 * sign, 8)

    def copy(number, src, dst, device):
        return pltpu.make_async_remote_copy(
            src_ref=src, dst_ref=dst, send_sem=ssem.at[number], recv_sem=rsem.at[number],
            device_id=device, device_id_type=MESH,
        )

    def others(k):
        return (sp, (tp + k) % NTP)

    def rows_of(t):
        return pl.ds(ROWS * t, ROWS)

    loads = [
        pltpu.make_async_copy(src, dst, isem.at[i])
        for i, (src, dst) in enumerate((
            (lat_hbm, lat_ref), (w_hbm, w_ref), (rot_hbm, krot.at[0]),
            (o_hbm, o_ref), (do_hbm, do_ref), (q_hbm, q_ref), (lse_hbm, lse_ref),
        ))
    ]
    barrier = pltpu.get_barrier_semaphore()
    greet = [dev(d, 0) for d in (4, -4, 1, -1, 2, -2)] + [dev(0, d) for d in (1, -1, 2)]
    greet += [others(k) for k in range(1, NTP)]
    for device in greet:
        pl.semaphore_signal(barrier, inc=1, device_id=device, device_id_type=MESH)
    for c in loads:
        c.start()
    mall[...] = jnp.zeros_like(mall)
    acc[...] = jnp.zeros_like(acc)

    for c in loads[0:3]:
        c.wait()
    kvm[0:ROWS, :] = dot(lat_ref[...], w_ref[...]).astype(BF16)
    latt[0] = jnp.transpose(lat_ref[...].astype(F32)).astype(BF16)

    for c in loads[3:7]:
        c.wait()
    delta = jnp.sum(o_ref[...].astype(F32) * do_ref[...].astype(F32), axis=0, keepdims=True)
    lse = lse_ref[...] * (1.0 / SCALE)
    row = lax.broadcasted_iota(jnp.int32, (16, ROWS), 0)
    aux = jnp.zeros((16, ROWS), F32)
    for i, piece in enumerate(three(lse) + three(delta)):
        aux = jnp.where(row == i, jnp.broadcast_to(piece, (16, ROWS)), aux)
    qbuf[0, 0:64, :] = q_ref[0:64, :]
    qbuf[0, 64:128, :] = do_ref[...]
    qbuf[0, 128:160, :] = q_ref[64:96, :]
    qbuf[0, 160:176, :] = aux.astype(BF16)

    pl.semaphore_wait(barrier, len(greet))

    mine = pl.ds(PART * tp, PART)
    far = [
        [
            copy(LAT + t - 1, latt.at[a, mine], latt.at[t, mine], device),
            copy(K_ROT + t - 1, krot.at[a], krot.at[t], device),
            copy(K_FAR + t - 1, kvm.at[rows_of(a)], kvm.at[rows_of(t)], device),
        ]
        for t, a, device in ((1, 0, dev(4 * sign, 0)), (2, 0, dev(-4 * sign, 0)), (3, 1, dev(4 * sign, 0)))
    ]
    q_n = [copy(Q_N + s - 1, qbuf.at[0], qbuf.at[4 * s], dev(n_off[s], 0)) for s in (1, 2, 3)]
    q_y = [
        [copy(Q_Y + 3 * s + u - 1, qbuf.at[4 * s], qbuf.at[4 * s + u], dev(0, y_off[u])) for u in (1, 2, 3)]
        for s in range(4)
    ]
    for c in q_n + q_y[0] + far[0] + far[1]:
        c.start()
    for s in (1, 2, 3):
        q_n[s - 1].wait_recv()
        for c in q_y[s]:
            c.start()

    lane = lax.broadcasted_iota(jnp.int32, (ROWS, 128), 1)
    marks = jnp.where((lane >= ROPE) & (lane < ROPE + 6), -1.0, 0.0)

    def prepare(t):
        here = slice(ROWS * t, ROWS * (t + 1))
        kt[0:64, here] = jnp.transpose(kvm[here, :].astype(F32))[0:64].astype(BF16)
        kt[64:96, here] = krot[t]
        rot_rows = jnp.concatenate([krot[t].astype(F32), jnp.zeros((ROWS - ROPE, ROWS), F32)], axis=0)
        kvx[here, :] = (jnp.transpose(rot_rows) + marks).astype(BF16)

    prepare(0)
    for i in range(3):
        far[0][i].wait_recv()
        far[2][i].start()
    for c in far[1]:
        c.wait_recv()
    share = [
        copy(LAT_TP + k - 1, latt.at[pl.ds(1, 2), mine], latt.at[pl.ds(1, 2), mine], others(k)) for k in range(1, NTP)
    ]
    for c in share:
        c.start()
    prepare(1)
    prepare(2)
    far[2][0].wait_recv()
    share_last = [copy(LAT_TP + 6 + k, latt.at[3, mine], latt.at[3, mine], others(k)) for k in range(1, NTP)]
    for c in share_last:
        c.start()

    def tile(s, first, count):
        m = mall[s]
        deltas = []
        for t in range(first, first + count):
            here = slice(ROWS * t, ROWS * (t + 1))
            both = dot(jnp.concatenate([kvm[here, :], kvx[here, :]], axis=1), m)
            ds, mixed = [], []
            for u in range(4):
                probs = jnp.exp2(both[:, 256 * u : 256 * u + 128] * (SCALE * LOG2E))
                ds.append((probs * both[:, 256 * u + 128 : 256 * u + 256]).astype(BF16))
                mixed += [ds[-1], probs.astype(BF16)]
            acc[here, :] += dot_nt(jnp.concatenate(mixed, axis=1), m)
            deltas.append(jnp.concatenate(ds, axis=1))
        deltas = deltas[0] if count == 1 else jnp.concatenate(deltas, axis=0)
        return dot(kt[:, ROWS * first : ROWS * (first + count)], deltas)

    def early(s, carry):
        for u in range(4):
            if u:
                copy(Q_Y + 3 * s + u - 1, qbuf.at[4 * s], qbuf.at[4 * s + u], dev(0, 1)).wait_recv()
            slot, at = 4 * s + u, 256 * u
            mall[s, 0:64, at : at + 128] = qbuf[slot, 0:64, :]
            mall[s, 64:128, at + 128 : at + 256] = qbuf[slot, 64:128, :]
            mall[s, 128:160, at : at + 128] = qbuf[slot, 128:160, :]
            extra = qbuf[slot, 160:176, :].astype(F32)
            mall[s, 160:176, at : at + 128] = jnp.where(row < 3, extra, 0.0).astype(BF16)
            mall[s, 160:176, at + 128 : at + 256] = jnp.where(row >= 3, extra, 0.0).astype(BF16)
        dqp[s] = tile(s, 0, 3)
        return carry

    lax.fori_loop(0, 4, early, 0)

    lane_scale = jnp.where(lane < NOPE, SCALE, 1.0)
    dkv, drot = [], []

    def finish(t):
        here = slice(ROWS * t, ROWS * (t + 1))
        main = acc[here, 0:128] * lane_scale
        hi = main.astype(BF16)
        rot_part = jnp.transpose(acc[here, 128:256])[0:ROPE] * SCALE
        if t == 0:
            rot_own[...] = rot_part
        else:
            rots[t - 1] = rot_part.astype(BF16)
            dkvs[t - 1] = hi
            owner = dev(-f_off[t], 0)
            drot.append(copy(DROT + t - 1, rots.at[t - 1], rotr.at[t - 1], owner))
            drot[-1].start()
            dkv.append(copy(DKV + t - 1, dkvs.at[t - 1], dkvr.at[t - 1], owner))
            dkv[-1].start()
        halves[here, 0:128] = hi
        halves[here, 128:256] = (main - hi.astype(F32)).astype(BF16)

    for t in (1, 2):
        finish(t)

    for c in far[2][1:]:
        c.wait_recv()
    prepare(3)

    def late(s, carry):
        total = dqp[s] + tile(s, 3, 1)
        dqp[s] = total
        for u in (1, 2, 3):
            dqb[4 * s + u] = total[:, 128 * u : 128 * u + 128].astype(BF16)
        return carry

    for s in range(4):
        late(s, 0)

    finish(3)
    finish(0)
    for c in share + share_last:
        c.wait_recv()
    wpart = dot(jnp.concatenate([latt[0], latt[1], latt[2], latt[3]], axis=1), halves[...])
    wpart = (wpart[:, 0:128] + wpart[:, 128:256]).reshape(NZ, NY, 8, 128)
    for v in range(NY):
        wsend[v] = wpart[:, v].reshape(NZ * 8, 128)
    wnarrow[...] = wsend[...].astype(BF16)
    w_y = []
    for u in (1, 2, 3):
        w_y.append(copy(W_Y + u - 1, wnarrow.at[(y + y_off[u] + NY) % NY], wrecv.at[u - 1], dev(0, y_off[u])))
        w_y[-1].start()

    dq_y = [
        [copy(DQ_Y + 3 * s + u - 1, dqb.at[4 * s + u], dqr.at[3 * s + u - 1], dev(0, -y_off[u])) for u in (1, 2, 3)]
        for s in range(4)
    ]
    for s in (3, 1, 2, 0):
        for c in dq_y[s]:
            c.start()

    def dq_sum(s):
        total = dqp[s, :, 0:128]
        for u in (1, 2, 3):
            dq_y[s][u - 1].wait_recv()
            total = total + dqr[3 * s + u - 1].astype(F32)
        return total

    for c in w_y:
        c.wait_recv()
    wsum = wsend[y]
    for u in range(3):
        wsum = wsum + wrecv[u].astype(F32)
    wzs[...] = wsum.reshape(NZ, 8, 128)
    wzb[...] = wzs[...].astype(BF16)
    w_z = []
    for d in (8, 7, 9, 6, 10, 5, 11, 4, 12, 3, 13, 2, 14, 1, 15):
        w_z.append(copy(W_Z + d - 1, wzb.at[(z + d) % NZ], wzr.at[d - 1], dev(d, 0)))
        w_z[-1].start()

    for c in drot:
        c.wait_recv()
    total = rot_own[...]
    for t in range(3):
        total = total + rotr[t].astype(F32)
    rotx[tp] = total.astype(BF16)
    rot = []
    for k in range(1, NTP):
        rot.append(copy(ROT + k - 1, rotx.at[tp], rotx.at[tp], others(k)))
        rot[-1].start()

    dq_n = []
    for s in (3, 1, 2):
        dqs[s - 1] = dq_sum(s)
        dq_n.append(copy(DQ_N + s - 1, dqs.at[s - 1], dqz.at[s - 1], dev(-n_off[s], 0)))
        dq_n[-1].start()

    for c in dkv:
        c.wait_recv()
    own = acc[0:ROWS, 0:128] * lane_scale
    for t in range(3):
        own = own + dkvr[t].astype(F32)
    own = jnp.transpose(own).astype(BF16)
    dk_ref[...] = own[0:NOPE]
    dv_ref[...] = own[NOPE:128]

    total = dq_sum(0)
    for c in dq_n:
        c.wait_recv()
    dq_ref[...] = ((total + dqz[0] + dqz[1] + dqz[2]) * SCALE).astype(BF16)

    for c in rot:
        c.wait_recv()
    total = rotx[0].astype(F32)
    for k in range(1, NTP):
        total = total + rotx[k].astype(F32)
    drot_ref[...] = total

    for c in w_z:
        c.wait_recv()
    wsum = wzs[z]
    for d in range(1, NZ):
        wsum = wsum + wzr[d - 1].astype(F32)
    dw_ref[...] = wsum

    for c in q_n + share + share_last + dkv + drot + w_y + w_z + rot + dq_n:
        c.wait_send()
    for group in far + q_y + dq_y:
        for c in group:
            c.wait_send()


def hand_over(*refs):
    for src, dst in zip(refs[:5], refs[5:]):
        dst[...] = src[...]


def per_device(queries, latents, rot_key, kv_weight, log_sums, outputs, out_grad):
    vmem = pl.BlockSpec(memory_space=pltpu.VMEM)
    shape = jax.ShapeDtypeStruct
    results = (
        shape((NOPE + ROPE, ROWS), BF16),
        shape((NOPE, ROWS), BF16),
        shape((VAL, ROWS), BF16),
        shape((ROPE, ROWS), F32),
        shape((8, 128), F32),
    )
    made = pl.pallas_call(
        kernel,
        out_shape=results,
        in_specs=[pl.BlockSpec(memory_space=pl.ANY)] * 7,
        out_specs=(vmem,) * 5,
        scratch_shapes=[
            pltpu.VMEM((NOPE + ROPE, ROWS), BF16),
            pltpu.VMEM((ROWS, RANK), BF16),
            pltpu.VMEM((RANK, 128), BF16),
            pltpu.VMEM((1, ROWS), F32),
            pltpu.VMEM((VAL, ROWS), BF16),
            pltpu.VMEM((VAL, ROWS), BF16),
            pltpu.VMEM((16, PACK, ROWS), BF16),
            pltpu.VMEM((4 * ROWS, 128), BF16),
            pltpu.VMEM((4 * ROWS, 128), BF16),
            pltpu.VMEM((4, ROPE, ROWS), BF16),
            pltpu.VMEM((96, 4 * ROWS), BF16),
            pltpu.VMEM((4, RANK, ROWS), BF16),
            pltpu.VMEM((4, 256, 1024), BF16),
            pltpu.VMEM((4 * ROWS, 256), F32),
            pltpu.VMEM((4, 96, 4 * ROWS), F32),
            pltpu.VMEM((16, 96, ROWS), BF16),
            pltpu.VMEM((12, 96, ROWS), BF16),
            pltpu.VMEM((3, 96, ROWS), F32),
            pltpu.VMEM((3, 96, ROWS), F32),
            pltpu.VMEM((3, ROWS, 128), BF16),
            pltpu.VMEM((3, ROWS, 128), BF16),
            pltpu.VMEM((4 * ROWS, 256), BF16),
            pltpu.VMEM((ROPE, ROWS), F32),
            pltpu.VMEM((3, ROPE, ROWS), BF16),
            pltpu.VMEM((3, ROPE, ROWS), BF16),
            pltpu.VMEM((NTP, ROPE, ROWS), BF16),
            pltpu.VMEM((NY, NZ * 8, 128), F32),
            pltpu.VMEM((NY, NZ * 8, 128), BF16),
            pltpu.VMEM((3, NZ * 8, 128), BF16),
            pltpu.VMEM((NZ, 8, 128), F32),
            pltpu.VMEM((NZ, 8, 128), BF16),
            pltpu.VMEM((NZ - 1, 8, 128), BF16),
            pltpu.SemaphoreType.DMA((7,)),
            pltpu.SemaphoreType.DMA((COPIES,)),
            pltpu.SemaphoreType.DMA((COPIES,)),
        ],
        compiler_params=pltpu.CompilerParams(collective_id=0, has_side_effects=True),
    )(queries.T, latents, rot_key.T, kv_weight, log_sums.T, outputs.T, out_grad.T)
    dq, dk, dv, drot, dw = pl.pallas_call(
        hand_over, out_shape=results, in_specs=[vmem] * 5, out_specs=(vmem,) * 5
    )(*made)
    return dq.T, dk.T, dv.T, drot.T, dw


def solution(mesh):
    placed = (
        P("sp", "tp"),
        P("sp", None),
        P("sp", None),
        P(None, "tp"),
        P("sp", "tp"),
        P("sp", "tp"),
        P("sp", "tp"),
    )
    return jax.shard_map(
        per_device,
        mesh=mesh,
        in_specs=placed,
        out_specs=(P("sp", "tp"), P("sp", "tp"), P("sp", "tp"), P("sp", None), P("sp", "tp")),
        check_vma=False,
    )
```
